512 devices in a mesh: kv: 16 (over y, x), tp: 32 (over z, core).
Axes of the slice: x: 4, y: 4, z: 16, core: 2. Of those that a mesh axis runs over, the one named last changes fastest.
Arguments:
- tokens: bfloat16 [3, 4096], P(None, ('kv', 'tp')), may hold values from -40 to 40
- lengths: int32 [3], replicated, may hold values from 1 to 131072, as said below
- attn_gain: float32 [4096], P(('kv', 'tp')), may hold values from 0.1 to 1.9
- w_query: bfloat16 [4096, 2048], P('kv', 'tp'), may hold values from -0.09375 to 0.09375
- w_key: bfloat16 [4096, 128], P('kv'), may hold values from -0.09375 to 0.09375
- w_value: bfloat16 [4096, 128], P('kv'), may hold values from -0.09375 to 0.09375
- w_forget: bfloat16 [4096, 32], replicated, may hold values from -0.09375 to 0.09375
- forget_bias: float32 [32], replicated, may hold values from -4 to 0
- cache_keys: bfloat16 [3, 128, 131072], P(None, None, ('kv', 'tp')), may hold values from -320 to 320
- cache_values: bfloat16 [3, 128, 131072], P(None, None, ('kv', 'tp')), may hold values from -6 to 6
- cache_decay: float32 [3, 32, 131072], P(None, None, ('kv', 'tp')), may hold values from -16388 to 0, as said below
- out_gain: float32 [2048], replicated, may hold values from 0.1 to 1.9
- w_out: bfloat16 [2048, 4096], P('tp', 'kv'), may hold values from -0.125 to 0.125
- mlp_gain: float32 [4096], P(('kv', 'tp')), may hold values from 0.1 to 1.9
- w_gate: bfloat16 [4096, 11264], P('kv', 'tp'), may hold values from -0.09375 to 0.09375
- w_up: bfloat16 [4096, 11264], P('kv', 'tp'), may hold values from -0.09375 to 0.09375
- w_down: bfloat16 [11264, 4096], P('tp', 'kv'), may hold values from -0.0546875 to 0.0546875
Outputs:
- layer_out: bfloat16 [3, 4096], P(None, ('kv', 'tp'))
The draws below stay inside these ranges and needn't reach their ends.
Inputs may be any that keep to these rules, and one draw needn't show every extreme that they name: Sequence b has lengths[b] live cache positions, 0 to lengths[b] - 1; some sequence has exactly 131072 in every draw. On live positions, cache_decay[b, h, j] is the sum of the log forget gates of sequence b and head h over positions j + 1 to lengths[b] - 1, so it is zero at the last live position and never rises toward earlier positions; it is zero beyond lengths[b].
All inputs are finite; a program needn't handle non-finite values.
Results may differ from the reference program's by a relative error of at most 0.013.
Values may be sent and summed in bfloat16 or wider, within the bound.
A program may use at most 64 MiB of HBM per device.

```python
import math
import jax
import jax.numpy as jnp
from jax import lax

D = 4096
QUERY_HEAD_COUNT = 32
HD = 64
KV_HEADS = 2
FF = 11264
SEQUENCE_COUNT = 3
LEN_DEV = 256
LEN = 131072
KV_COLS = 256


def lengths_of(key):
    folded = jax.random.fold_in(key, 101)
    key_shift, key_cut, key_full = jax.random.split(folded, 3)
    shifts = jax.random.randint(key_shift, (SEQUENCE_COUNT,), 0, 6)
    longest = jnp.right_shift(jnp.full((SEQUENCE_COUNT,), LEN, jnp.int32), shifts)
    cut_off = jax.random.randint(key_cut, (SEQUENCE_COUNT,), 0, longest // 2 + 1)
    sequence_length = jnp.maximum(longest - cut_off, 1)
    chosen = jax.random.randint(key_full, (), 0, SEQUENCE_COUNT)
    return jnp.where(jnp.arange(SEQUENCE_COUNT) == chosen, LEN, sequence_length).astype(jnp.int32)


def draw_lengths(key, part):
    return lengths_of(key)


def draw_cache_decay(key, part):
    sequence_length = lengths_of(key)
    folded = jax.random.fold_in(key, 202)
    key_kind, key_block, key_rough, key_location, key_dimension = jax.random.split(folded, 5)
    lagging_heads = (jax.random.randint(key_kind, (QUERY_HEAD_COUNT,), 0, 2) == 1).astype(jnp.float32)
    base_rate = lagging_heads / LEN + (1.0 - lagging_heads) / 40.0
    log_two = math.log(2.0)
    blocks = LEN // LEN_DEV
    block_factor = jnp.exp(jax.random.uniform(key_block, (QUERY_HEAD_COUNT, blocks), jnp.float32, -log_two, log_two))
    block_factor = jnp.repeat(block_factor, LEN_DEV, axis=1)
    roughness = jnp.exp(jax.random.uniform(key_rough, (SEQUENCE_COUNT, QUERY_HEAD_COUNT, LEN), jnp.float32, -log_two, log_two))
    step_amount = base_rate[None, :, None] * block_factor[None] * roughness
    spike_locations = jax.random.randint(key_location, (SEQUENCE_COUNT, QUERY_HEAD_COUNT, 3), 0, sequence_length[:, None, None])
    spike_penalty = jax.random.uniform(key_dimension, (SEQUENCE_COUNT, QUERY_HEAD_COUNT, 3), jnp.float32, 0.2, 0.5)
    spike_offset = -jnp.log(1.0 - spike_penalty) * lagging_heads[None, :, None]
    token_positions = jnp.arange(LEN)
    for spike_index in range(3):
        match_found = token_positions[None, None, :] == spike_locations[:, :, spike_index:spike_index + 1]
        step_amount = step_amount + jnp.where(match_found, spike_offset[:, :, spike_index:spike_index + 1], 0.0)
    running = jnp.cumsum(step_amount, axis=2)
    newest = jnp.broadcast_to((sequence_length - 1)[:, None, None], (SEQUENCE_COUNT, QUERY_HEAD_COUNT, 1))
    at_newest = jnp.take_along_axis(running, newest, axis=2)
    return jnp.where(token_positions[None, None, :] < sequence_length[:, None, None], running - at_newest, 0.0).astype(jnp.float32)


def draw_cache_keys(key, part):
    folded = jax.random.fold_in(key, 303)
    key_base = jax.random.fold_in(folded, 0)
    full_shape = (SEQUENCE_COUNT, KV_HEADS, HD, LEN)
    entries = jnp.clip(jax.random.normal(key_base, full_shape, jnp.float32), -6.0, 6.0)
    return entries.reshape(SEQUENCE_COUNT, KV_HEADS * HD, LEN).astype(jnp.bfloat16)


def draw_tokens(key, part):
    folded = jax.random.fold_in(key, 404)
    key_value = jax.random.fold_in(folded, 0)
    column = jnp.arange(D)
    inside = (column % KV_COLS).astype(jnp.float32) / KV_COLS
    log_three = math.log(3.0)
    column_scale = 0.4 * jnp.exp(log_three * column.astype(jnp.float32) / D + log_three * inside)
    entries = jnp.clip(jax.random.normal(key_value, (SEQUENCE_COUNT, D), jnp.float32), -6.0, 6.0)
    return (entries * column_scale[None, :]).astype(jnp.bfloat16)


def shard_levels(stream_key, dims, cuts, least, largest):
    def one(dim, shards_of):
        heights = jax.random.uniform(jax.random.fold_in(jax.random.fold_in(stream_key, 6), dim), (shards_of,), jnp.float32, least / len(cuts), largest / len(cuts))
        return jnp.repeat(jnp.exp(heights), dims[dim] // shards_of).reshape((-1,) + (1,) * (len(dims) - dim - 1))

    gain = one(*cuts[0])
    for cut in cuts[1:]:
        gain = gain * one(*cut)
    return gain


def noise(stream_key, shape, width, limit, cuts=(), kind=jnp.bfloat16):
    factor_of = shard_levels(stream_key, shape, cuts, -0.22, 0.18) if cuts else 1.0
    result = jax.random.normal(stream_key, shape, jnp.float32) * width * factor_of
    return jnp.minimum(jnp.maximum(result, -limit), limit).astype(kind)


def setup_inputs(seed: int = 0) -> dict:
    seeds = jax.random.split(jax.random.key(seed), 18)
    return {
        "tokens": draw_tokens(jax.random.fold_in(seeds[17], 71), 0),
        "lengths": draw_lengths(jax.random.fold_in(seeds[17], 71), 0),
        "attn_gain": jnp.clip(1.0 + 0.18 * jax.random.normal(seeds[2], (D,), jnp.float32), 0.1, 1.9),
        "w_query": noise(seeds[3], (D, QUERY_HEAD_COUNT * HD), D ** -0.5, 0.09375, ((0, 16), (1, 32))),
        "w_key": noise(seeds[4], (D, KV_HEADS * HD), D ** -0.5, 0.09375, ((0, 16),)),
        "w_value": noise(seeds[5], (D, KV_HEADS * HD), D ** -0.5, 0.09375, ((0, 16),)),
        "w_forget": noise(seeds[6], (D, QUERY_HEAD_COUNT), D ** -0.5, 0.09375),
        "forget_bias": jnp.clip(jax.random.uniform(seeds[7], (QUERY_HEAD_COUNT,), jnp.float32, -4.0, 0.0), -4.0, 0.0),
        "cache_keys": draw_cache_keys(jax.random.fold_in(seeds[17], 71), 0),
        "cache_values": noise(seeds[9], (SEQUENCE_COUNT, KV_HEADS * HD, LEN), 1.0, 6.0, ((2, 512),)),
        "cache_decay": draw_cache_decay(jax.random.fold_in(seeds[17], 71), 0),
        "out_gain": jnp.clip(1.0 + 0.18 * jax.random.normal(seeds[11], (QUERY_HEAD_COUNT * HD,), jnp.float32), 0.1, 1.9),
        "w_out": noise(seeds[12], (QUERY_HEAD_COUNT * HD, D), (QUERY_HEAD_COUNT * HD) ** -0.5, 0.125, ((0, 32), (1, 16))),
        "mlp_gain": jnp.clip(1.0 + 0.18 * jax.random.normal(seeds[13], (D,), jnp.float32), 0.1, 1.9),
        "w_gate": noise(seeds[14], (D, FF), D ** -0.5, 0.09375, ((0, 16), (1, 32))),
        "w_up": noise(seeds[15], (D, FF), D ** -0.5, 0.09375, ((0, 16), (1, 32))),
        "w_down": noise(seeds[16], (FF, D), FF ** -0.5, 0.0546875, ((0, 32), (1, 16))),
    }


epsilon = 1e-06
masked_score = -1e+30

def inverse_rms(rows):
    values = rows.astype(jnp.float32)
    return lax.rsqrt(lax.optimization_barrier(jnp.mean(values * values, axis=1, keepdims=True)) + epsilon)

def attend_sequence(items):
    query_row, key_row, value_row, keys_seq, values_seq, decay_seq, gate_row, length_one = items
    groups = QUERY_HEAD_COUNT // KV_HEADS
    score_scale = HD ** (-0.5)
    query_grouped = query_row.astype(jnp.float32).reshape(KV_HEADS, groups, HD)
    keys_grouped = keys_seq.astype(jnp.float32).reshape(KV_HEADS, HD, LEN)
    values_grouped = values_seq.astype(jnp.float32).reshape(KV_HEADS, HD, LEN)
    scores = jnp.einsum('kgd,kdj->kgj', query_grouped, keys_grouped).reshape(QUERY_HEAD_COUNT, LEN)
    scores = scores * score_scale + decay_seq + gate_row[:, None]
    is_live = (jnp.arange(LEN, dtype=jnp.int32) < length_one)[None, :]
    scores = jnp.where(is_live, scores, masked_score)
    own_score = jnp.einsum('kgd,kd->kg', query_grouped, key_row.astype(jnp.float32).reshape(KV_HEADS, HD)).reshape(QUERY_HEAD_COUNT) * score_scale
    score_top = jnp.maximum(lax.optimization_barrier(jnp.max(scores, axis=1)), own_score)
    weights = jnp.where(is_live, jnp.exp(scores - score_top[:, None]), 0.0)
    own_weight = jnp.exp(own_score - score_top)
    weight_total = lax.optimization_barrier(jnp.sum(weights, axis=1)) + own_weight
    rounded = lax.optimization_barrier(weights.astype(jnp.bfloat16)).astype(jnp.float32)
    value_sums = jnp.einsum('kgj,kdj->kgd', rounded.reshape(KV_HEADS, groups, LEN), values_grouped).reshape(QUERY_HEAD_COUNT, HD)
    new_values = jnp.repeat(value_row.astype(jnp.float32).reshape(KV_HEADS, HD), groups, axis=0)
    value_sums = value_sums + own_weight[:, None] * new_values
    return value_sums / weight_total[:, None]

def reference(tokens, lengths, attn_gain, w_query, w_key, w_value, w_forget, forget_bias, cache_keys, cache_values, cache_decay, out_gain, w_out, mlp_gain, w_gate, w_up, w_down):
    batch_rows = tokens.shape[0]
    first_rms = inverse_rms(tokens)
    scaled_one = (tokens.astype(jnp.float32) * attn_gain).astype(jnp.bfloat16)
    query = (jnp.dot(scaled_one, w_query, preferred_element_type=jnp.float32) * first_rms).astype(jnp.bfloat16)
    key_new = (jnp.dot(scaled_one, w_key, preferred_element_type=jnp.float32) * first_rms).astype(jnp.bfloat16)
    value_new = (jnp.dot(scaled_one, w_value, preferred_element_type=jnp.float32) * first_rms).astype(jnp.bfloat16)
    log_gate = jax.nn.log_sigmoid(jnp.dot(scaled_one, w_forget, preferred_element_type=jnp.float32) * first_rms + forget_bias)
    heads_out = lax.map(attend_sequence, (query, key_new, value_new, cache_keys, cache_values, cache_decay, log_gate, lengths))
    normed = heads_out * lax.rsqrt(lax.optimization_barrier(jnp.mean(heads_out * heads_out, axis=2, keepdims=True)) + epsilon) * out_gain.reshape(QUERY_HEAD_COUNT, HD)
    normed = normed.astype(jnp.bfloat16).reshape(batch_rows, QUERY_HEAD_COUNT * HD)
    residual = (tokens.astype(jnp.float32) + jnp.dot(normed, w_out, preferred_element_type=jnp.float32)).astype(jnp.bfloat16)
    second_rms = inverse_rms(residual)
    scaled_two = (residual.astype(jnp.float32) * mlp_gain).astype(jnp.bfloat16)
    gate = jnp.dot(scaled_two, w_gate, preferred_element_type=jnp.float32) * second_rms
    up_part = jnp.dot(scaled_two, w_up, preferred_element_type=jnp.float32) * second_rms
    hidden = (jax.nn.silu(gate) * up_part).astype(jnp.bfloat16)
    return (residual.astype(jnp.float32) + jnp.dot(hidden, w_down, preferred_element_type=jnp.float32)).astype(jnp.bfloat16)
```

```python
import jax
import jax.numpy as jnp
from jax import lax
from jax.experimental import pallas as pl
from jax.experimental.pallas import tpu as pltpu
from jax.sharding import PartitionSpec as P

MESH = pl.DeviceIdType.MESH
D = 4096
HD = 64
NTP = 32
NKV = 16
FF_DEV = 352
FF_PAD = 384
SPAN = 256
EPS = 1e-06
MASKED = -1e30
F32 = jnp.float32
BF16 = jnp.bfloat16

NT = (((1,), (1,)), ((), ()))
NN = (((1,), (0,)), ((), ()))

Z_ORDER = [8, 7, -7, 6, -6, 5, -5, 4, -4, 3, -3, 2, -2, 1, -1]


def dot(a, b, dims, **kw):
    return lax.dot_general(a, b, dims, preferred_element_type=F32, **kw)


def iota(shape, dim):
    return lax.broadcasted_iota(jnp.int32, shape, dim)


def kernel(
    lengths, tokens, attn_gain, mlp_gain, forget_bias, out_gain,
    w_query, w_key, w_value, w_forget, keys, values, decay, w_out,
    w_gate, w_up, w_down,
    out,
    tok_v, ag_v, mg_v, fb_v, og_v, wqf, wk, wv, wkv, k_v, v_v, d_v, wo,
    wg, wu, wd,
    buf1, buf2, buf3, stage4, buf4, buf5, buf6, buf7, stage8, buf8,
    lsem, ssem, rsem,
):
    kv = lax.axis_index("kv")
    tp = lax.axis_index("tp")
    g = tp // 16
    z = tp // 2
    core = tp % 2
    y = kv // 4
    x = kv % 4

    def load(i, src, dst):
        c = pltpu.make_async_copy(src, dst, lsem.at[i])
        c.start()
        return c

    half = pl.multiple_of(g * HD, HD)
    other = pl.multiple_of((1 - g) * HD, HD)
    c_tok = load(0, tokens, tok_v)
    c_ag = load(1, attn_gain, ag_v)
    c_mg = load(2, mlp_gain, mg_v)
    c_wq = load(3, w_query, wqf.at[pl.ds(half, HD)])
    cols = pl.ds(pl.multiple_of(kv * 256, 256), 256)
    c_wf = load(4, w_forget.at[:, cols], wqf.at[pl.ds(other, 32)])
    c_wk = load(5, w_key, wk)
    c_wv = load(6, w_value, wv)
    c_k = load(7, keys, k_v)
    c_d = load(8, decay, d_v)
    c_v = load(9, values, v_v)
    c_fb = load(10, forget_bias, fb_v)
    c_og = load(11, out_gain, og_v)
    c_wo = load(12, w_out, wo.at[pl.ds(half, HD)])
    c_wg = load(13, w_gate, wg.at[pl.ds(0, FF_DEV)])
    c_wu = load(14, w_up, wu.at[pl.ds(0, FF_DEV)])
    c_wd = load(15, w_down, wd.at[pl.ds(0, FF_DEV)])

    tp_peers = []
    for dz in Z_ORDER:
        zz = lax.rem(z + (dz + 16), 16)
        for dc in (0, 1):
            cc = core if dc == 0 else 1 - core
            tp_peers.append(zz * 2 + cc)
    tp_peers.append(z * 2 + (1 - core))
    kv_peers = []
    for dist in (4, 3, 2, 1):
        for dy in (2, 1, 3, 0):
            for dx in (2, 1, 3, 0):
                if min(dy, 4 - dy) + min(dx, 4 - dx) == dist:
                    kv_peers.append(lax.rem(y + dy, 4) * 4 + lax.rem(x + dx, 4))

    barrier = pltpu.get_barrier_semaphore()
    for p in tp_peers:
        pl.semaphore_signal(barrier, inc=1, device_id={"tp": p}, device_id_type=MESH)
    for p in kv_peers:
        pl.semaphore_signal(barrier, inc=1, device_id={"kv": p}, device_id_type=MESH)

    def send(n, axis, peers, src, dst):
        for p in peers:
            pltpu.make_async_remote_copy(
                src_ref=src(p), dst_ref=dst, send_sem=ssem.at[n], recv_sem=rsem.at[n],
                device_id={axis: p}, device_id_type=MESH,
            ).start()

    def arrived(n, ref):
        pltpu.make_async_copy(ref, ref, rsem.at[n]).wait()

    def sent(n, ref):
        pltpu.make_async_copy(ref, ref, ssem.at[n]).wait()

    lane8 = iota((8, 128), 1)
    row8 = iota((8, 128), 0)
    lane1 = iota((1, 128), 1)
    ghalf8 = (lane8 // HD) == g
    mlane = (1 - g) * HD

    c_tok.wait()
    c_ag.wait()
    c_mg.wait()
    tok = tok_v[...].astype(F32)
    scaled = (tok * ag_v[...]).astype(BF16).astype(F32)
    row = jnp.concatenate(
        [scaled[0:1], scaled[1:2], scaled[2:3], tok[0:1], tok[1:2], tok[2:3], mg_v[...],
         jnp.zeros((1, 72), F32)], axis=1)
    buf1[pl.ds(tp, 1)] = row.reshape(1, 1, 128)

    wqf[pl.ds(other + 32, 32)] = jnp.zeros((32, 256), BF16)
    wo[pl.ds(other, HD)] = jnp.zeros((HD, 256), BF16)
    for w in (wg, wu, wd):
        w[FF_DEV:] = jnp.zeros((FF_PAD - FF_DEV, 256), BF16)
    c_wk.wait()
    c_wv.wait()
    wkv[...] = jnp.where(
        (iota((256, 128), 1) // HD) == g,
        wk[...].astype(F32), pltpu.roll(wv[...].astype(F32), HD, 1)).astype(BF16)
    c_wq.wait()
    c_wf.wait()

    pl.semaphore_wait(barrier, len(tp_peers) + len(kv_peers))
    send(0, "tp", tp_peers, lambda p: buf1.at[tp], buf1.at[tp])
    r24 = iota((24, 128), 0)
    b24 = r24 % 4
    want24 = jnp.where(
        r24 < 16,
        jnp.where((r24 < 4) | ((r24 >= 12) & (r24 < 16)), b24, -1),
        b24 + 3)
    l24 = iota((24, 128), 1)
    sel = jnp.where((b24 < 3) & (l24 // 8 == want24), 1.0, 0.0).astype(BF16)
    spread = (iota((256, 128), 0) % 8) == (iota((256, 128), 1) % 8)
    arrived(0, buf1.at[pl.ds(0, NTP - 1)])
    block = jnp.broadcast_to(buf1[...], (NTP, 8, 128)).reshape(256, 128)
    block = jnp.where(spread, block, 0.0)
    rows = dot(sel, block.astype(BF16), NT)
    tok_rows = rows[16:24]
    part = dot(rows[0:8].astype(BF16), wqf[...], NT) + dot(rows[8:16].astype(BF16), wkv[...], NN)
    squares = jnp.sum(tok_rows * tok_rows, axis=1, keepdims=True)
    part = jnp.where((lane8 == mlane + 32) & (row8 < 4), squares, part)
    buf2[pl.ds(kv, 1)] = part.reshape(1, 8, 128)
    send(1, "kv", kv_peers, lambda p: buf2.at[kv], buf2.at[kv])

    tok8 = jnp.where(row8 < 4, tok_rows[:, :128], tok_rows[:, 128:])
    gsel = jnp.where(lane8 // 8 == 6, 1.0, 0.0)
    gain_rows = dot(gsel, block, NT, precision=lax.Precision.HIGHEST)
    gain8 = jnp.where(row8 < 4, gain_rows[:, :128], gain_rows[:, 128:])
    c_fb.wait()
    c_og.wait()
    bias_row = jnp.concatenate([fb_v[...], jnp.zeros((1, 96), F32)], axis=1)
    bias = jnp.sum(jnp.where(lane1 == tp, bias_row, 0.0), axis=1, keepdims=True)
    og = og_v[pl.ds(z, 1)]
    og = jnp.where(core == g, og, pltpu.roll(og, HD, 1))

    arrived(1, buf2.at[pl.ds(0, NKV - 1)])
    total8 = jnp.sum(buf2[...], axis=0)
    sq = jnp.sum(jnp.where(lane8 == mlane + 32, total8, 0.0), axis=1, keepdims=True)
    rms1 = lax.rsqrt(sq * (1.0 / D) + EPS)
    q8 = jnp.where(ghalf8 & (row8 < 3), (total8 * rms1).astype(BF16).astype(F32), 0.0)
    for b in range(3):
        buf3[b, pl.ds(tp, 1)] = q8[b:b + 1].reshape(1, 1, 128)
    send(2, "tp", tp_peers, lambda p: buf3.at[:, tp], buf3.at[:, tp])

    kv8 = (pltpu.roll(total8, 4, 0) * rms1).astype(BF16).astype(F32)
    own = jnp.sum(q8 * kv8, axis=1, keepdims=True) * (HD ** -0.5)
    v8 = pltpu.roll(kv8, HD, 1)
    fj = jnp.sum(jnp.where(lane8 == mlane + tp, total8, 0.0), axis=1, keepdims=True) * rms1 + bias
    log_gate = jnp.minimum(fj, 0.0) - jnp.log1p(jnp.exp(-jnp.abs(fj)))
    c_k.wait()
    c_d.wait()
    c_v.wait()
    positions = (kv * NTP + tp) * SPAN + iota((32, SPAN), 1)
    lane32 = iota((32, 128), 1)
    ghalf32 = (lane32 // HD) == (iota((32, 128), 0) // 16)
    mlane32 = (1 - iota((32, 128), 0) // 16) * HD

    arrived(2, buf3.at[:, pl.ds(0, NTP - 1)])
    for b in range(3):
        qb = buf3[b].reshape(32, 128).astype(BF16)
        s = dot(qb, k_v[b], NN) * (HD ** -0.5) + d_v[b]
        live = positions < lengths[b]
        s = jnp.where(live, s, MASKED)
        top = jnp.max(s, axis=1, keepdims=True)
        w = jnp.where(live, jnp.exp(s - top), 0.0)
        tot = jnp.sum(w, axis=1, keepdims=True)
        vs = dot(w.astype(BF16), v_v[b], NT)
        msg = jnp.where(ghalf32, vs, jnp.where(lane32 == mlane32, top, tot))
        stage4[b] = msg.reshape(32, 1, 128)
    buf4[:, pl.ds(tp, 1)] = stage4[:, pl.ds(tp, 1)]
    send(3, "tp", tp_peers, lambda p: stage4.at[:, p], buf4.at[:, tp])

    def merge(y2):
        n = y2.shape[0]
        at_m = iota((n, 128), 1) == mlane
        m = jnp.sum(jnp.where(at_m, y2, 0.0), axis=1, keepdims=True)
        top2 = jnp.max(m, axis=0, keepdims=True)
        zsum = jnp.sum(jnp.exp(m - top2) * y2, axis=0, keepdims=True)
        return jnp.where(lane1 == mlane, top2, zsum)

    c_wo.wait()
    arrived(3, buf4.at[:, pl.ds(0, NTP - 1)])
    for b in range(3):
        buf5[b, pl.ds(kv, 1)] = merge(buf4[b].reshape(NTP, 128)).reshape(1, 1, 128)
    send(4, "kv", kv_peers, lambda p: buf5.at[:, kv], buf5.at[:, kv])
    arrived(4, buf5.at[:, pl.ds(0, NKV - 1)])
    zrow = jnp.concatenate(
        [merge(buf5[b].reshape(NKV, 128)) for b in range(3)] + [jnp.ones((5, 128), F32)], axis=0)
    m8 = jnp.sum(jnp.where(lane8 == mlane, zrow, 0.0), axis=1, keepdims=True) + log_gate
    l8 = jnp.sum(jnp.where(lane8 == mlane + 1, zrow, 0.0), axis=1, keepdims=True)
    top8 = jnp.maximum(m8, own)
    a8 = jnp.exp(m8 - top8)
    o8 = jnp.exp(own - top8)
    heads = (zrow * a8 + o8 * v8) / (l8 * a8 + o8)
    heads = jnp.where(ghalf8 & (row8 < 3), heads, 0.0)
    mean = jnp.sum(heads * heads, axis=1, keepdims=True) * (1.0 / HD)
    normed = heads * lax.rsqrt(mean + EPS) * og
    n_lo = normed.astype(BF16)
    n_hi = pltpu.roll(normed, 4, 0).astype(BF16)
    attn = dot(n_lo, wo[:, :128], NN) + dot(n_hi, wo[:, 128:], NN)
    buf6[pl.ds(tp, 1)] = attn.astype(BF16).reshape(1, 8, 128)
    send(5, "tp", tp_peers, lambda p: buf6.at[tp], buf6.at[tp])
    c_wg.wait()
    c_wu.wait()
    c_wd.wait()
    arrived(5, buf6.at[pl.ds(0, NTP - 1)])
    attn8 = jnp.sum(buf6[...].astype(F32), axis=0)
    res8 = (tok8 + attn8).astype(BF16).astype(F32)
    sc8 = (res8 * gain8).astype(BF16).astype(F32)
    sw8 = pltpu.roll(sc8, 4, 0)
    low = row8 < 4
    lhs_g = jnp.concatenate([jnp.where(low, sc8, 0.0), jnp.where(low, sw8, 0.0)], axis=1).astype(BF16)
    lhs_u = jnp.concatenate([jnp.where(low, 0.0, sw8), jnp.where(low, 0.0, sc8)], axis=1).astype(BF16)
    gu = dot(lhs_g, wg[...], NT) + dot(lhs_u, wu[...], NT)
    sq2 = jnp.sum(res8 * res8, axis=1, keepdims=True) + jnp.zeros((8, 128), F32)
    sq2 = sq2 + pltpu.roll(sq2, 4, 0)
    sq2_hi = sq2.astype(BF16).astype(F32)
    lane_t = lane8 + 256
    tail = jnp.where(lane_t == FF_DEV, sq2_hi, jnp.where(lane_t == FF_DEV + 1, sq2 - sq2_hi, gu[:, 256:]))
    gu = jnp.concatenate([gu[:, :256], tail], axis=1)
    buf7[pl.ds(kv, 1)] = gu.astype(BF16).reshape(1, 8, FF_PAD)
    send(6, "kv", kv_peers, lambda p: buf7.at[kv], buf7.at[kv])

    i64 = iota((64, 256), 0)
    n64 = iota((64, 256), 1)
    res_rows = jnp.concatenate([res8, pltpu.roll(res8, 4, 0)], axis=1)
    rep = jnp.broadcast_to(res_rows.reshape(8, 1, 256), (8, 8, 256)).reshape(64, 256)
    diag = (i64 % 8) == (n64 % 8)
    mine = jnp.where(iota((8, 256), 1) // 8 == tp, 1.0, 0.0).astype(BF16)
    res_mine = dot(mine, jnp.where(diag, rep, 0.0).astype(BF16), NT)[0:1]
    fold = jnp.where(iota((32, 256), 1) // 8 == iota((32, 256), 0), 1.0, 0.0).astype(BF16)

    arrived(6, buf7.at[pl.ds(0, NKV - 1)])
    gs = jnp.sum(buf7[...].astype(F32), axis=0)
    tail = gs[:, 256:]
    sq2 = jnp.sum(
        jnp.where((lane_t == FF_DEV) | (lane_t == FF_DEV + 1), tail, 0.0), axis=1, keepdims=True)
    rms2 = lax.rsqrt(sq2 * (1.0 / D) + EPS)
    gs = gs * jnp.concatenate([rms2[0:4], rms2[0:4]], axis=0)
    up = pltpu.roll(gs, 4, 0)
    hid = gs / (1.0 + jnp.exp(-gs)) * up
    hid = jnp.where((iota((8, FF_PAD), 1) < FF_DEV) & (iota((8, FF_PAD), 0) < 3), hid, 0.0)
    hid = jnp.broadcast_to(hid.reshape(8, 1, FF_PAD), (8, 8, FF_PAD)).reshape(64, FF_PAD)
    down = dot(hid.astype(BF16), wd[...], NN)
    down = jnp.where(diag, down, 0.0)
    d_hi = down.astype(BF16)
    d_lo = (down - d_hi.astype(F32)).astype(BF16)
    parts = dot(fold, d_hi, NT) + dot(fold, d_lo, NT)
    parts = jnp.concatenate([parts, jnp.zeros((32, 64), F32)], axis=1)
    stage8[...] = parts.reshape(32, 1, 128)
    buf8[pl.ds(tp, 1)] = stage8[pl.ds(tp, 1)]
    send(7, "tp", tp_peers, lambda p: stage8.at[p], buf8.at[tp])
    arrived(7, buf8.at[pl.ds(0, NTP - 1)])
    share = jnp.sum(buf8[...], axis=0)[:, :64] + res_mine
    out[...] = jnp.concatenate([share[:, 0:8], share[:, 8:16], share[:, 16:24]], axis=0).astype(BF16)

    sent(0, buf1.at[pl.ds(0, NTP - 1)])
    sent(1, buf2.at[pl.ds(0, NKV - 1)])
    sent(2, buf3.at[:, pl.ds(0, NTP - 1)])
    sent(3, buf4.at[:, pl.ds(0, NTP - 1)])
    sent(4, buf5.at[:, pl.ds(0, NKV - 1)])
    sent(5, buf6.at[pl.ds(0, NTP - 1)])
    sent(6, buf7.at[pl.ds(0, NKV - 1)])
    sent(7, buf8.at[pl.ds(0, NTP - 1)])


def body(
    tokens, lengths, attn_gain, w_query, w_key, w_value, w_forget, forget_bias,
    cache_keys, cache_values, cache_decay, out_gain, w_out, mlp_gain, w_gate, w_up, w_down,
):
    hbm = pl.BlockSpec(memory_space=pl.ANY)
    v = pltpu.VMEM
    return pl.pallas_call(
        kernel,
        out_shape=jax.ShapeDtypeStruct((3, 8), BF16),
        in_specs=[pl.BlockSpec(memory_space=pltpu.SMEM)] + [hbm] * 16,
        out_specs=pl.BlockSpec(memory_space=pltpu.VMEM),
        scratch_shapes=[
            v((3, 8), BF16), v((1, 8), F32), v((1, 8), F32), v((1, 32), F32), v((16, 128), F32),
            v((128, 256), BF16), v((256, 128), BF16), v((256, 128), BF16), v((256, 128), BF16),
            v((3, 128, SPAN), BF16), v((3, 128, SPAN), BF16), v((3, 32, SPAN), F32),
            v((128, 256), BF16),
            v((FF_PAD, 256), BF16), v((FF_PAD, 256), BF16), v((FF_PAD, 256), BF16),
            v((NTP, 1, 128), F32), v((NKV, 8, 128), F32), v((3, NTP, 1, 128), F32),
            v((3, NTP, 1, 128), F32), v((3, NTP, 1, 128), F32), v((3, NKV, 1, 128), F32),
            v((NTP, 8, 128), BF16), v((NKV, 8, FF_PAD), BF16),
            v((NTP, 1, 128), F32), v((NTP, 1, 128), F32),
            pltpu.SemaphoreType.DMA((16,)),
            pltpu.SemaphoreType.DMA((8,)),
            pltpu.SemaphoreType.DMA((8,)),
        ],
        compiler_params=pltpu.CompilerParams(
            collective_id=0, has_side_effects=True, vmem_limit_bytes=60 * 1024 * 1024),
    )(
        lengths, tokens, attn_gain.reshape(1, 8), mlp_gain.reshape(1, 8),
        forget_bias.reshape(1, 32), out_gain.reshape(16, 128),
        w_query.T, w_key, w_value, w_forget.T, cache_keys, cache_values, cache_decay, w_out,
        w_gate.T, w_up.T, w_down,
    )


def solution(mesh):
    kvtp = ("kv", "tp")
    placed = (
        P(None, kvtp), P(), P(kvtp), P("kv", "tp"), P("kv", None), P("kv", None), P(), P(),
        P(None, None, kvtp), P(None, None, kvtp), P(None, None, kvtp), P(), P("tp", "kv"),
        P(kvtp), P("kv", "tp"), P("kv", "tp"), P("tp", "kv"),
    )
    return jax.shard_map(
        body, mesh=mesh, in_specs=placed, out_specs=P(None, kvtp), check_vma=False)
```

```python
import jax
import jax.numpy as jnp
from jax import lax
from jax.experimental import pallas as pl
from jax.experimental.pallas import tpu as pltpu
from jax.sharding import PartitionSpec as P

MESH = pl.DeviceIdType.MESH
D = 4096
HD = 64
NTP = 32
NKV = 16
FF_DEV = 352
FF_PAD = 384
SPAN = 256
EPS = 1e-06
MASKED = -1e30
F32 = jnp.float32
BF16 = jnp.bfloat16

NT = (((1,), (1,)), ((), ()))
NN = (((1,), (0,)), ((), ()))

Z_ORDER = [8, 7, -7, 6, -6, 5, -5, 4, -4, 3, -3, 2, -2, 1, -1]


def dot(a, b, dims, **kw):
    return lax.dot_general(a, b, dims, preferred_element_type=F32, **kw)


def iota(shape, dim):
    return lax.broadcasted_iota(jnp.int32, shape, dim)


def kernel(
    lengths, tokens, attn_gain, mlp_gain, forget_bias, out_gain,
    w_query, w_key, w_value, w_forget, keys, values, decay, w_out,
    w_gate, w_up, w_down,
    out,
    tok_v, ag_v, mg_v, fb_v, og_v, wqf, wk, wv, wkv, k_v, v_v, d_v, wo,
    wg, wu, wd,
    buf1, buf2, buf3, stage4, buf4, buf5, buf6, buf7, stage8, buf8,
    lsem, ssem, rsem,
):
    kv = lax.axis_index("kv")
    tp = lax.axis_index("tp")
    g = tp // 16
    z = tp // 2
    core = tp % 2
    y = kv // 4
    x = kv % 4

    def load(i, src, dst):
        c = pltpu.make_async_copy(src, dst, lsem.at[i])
        c.start()
        return c

    half = pl.multiple_of(g * HD, HD)
    other = pl.multiple_of((1 - g) * HD, HD)
    c_tok = load(0, tokens, tok_v)
    c_ag = load(1, attn_gain, ag_v)
    c_mg = load(2, mlp_gain, mg_v)
    c_wq = load(3, w_query, wqf.at[pl.ds(half, HD)])
    cols = pl.ds(pl.multiple_of(kv * 256, 256), 256)
    c_wf = load(4, w_forget.at[:, cols], wqf.at[pl.ds(other, 32)])
    c_wk = load(5, w_key, wk)
    c_wv = load(6, w_value, wv)
    c_k = load(7, keys, k_v)
    c_d = load(8, decay, d_v)
    c_v = load(9, values, v_v)
    c_fb = load(10, forget_bias, fb_v)
    c_og = load(11, out_gain, og_v)
    c_wo = load(12, w_out, wo.at[pl.ds(half, HD)])
    c_wg = load(13, w_gate, wg.at[pl.ds(0, FF_DEV)])
    c_wu = load(14, w_up, wu.at[pl.ds(0, FF_DEV)])
    c_wd = load(15, w_down, wd.at[pl.ds(0, FF_DEV)])

    tp_peers = []
    for dz in Z_ORDER:
        zz = lax.rem(z + (dz + 16), 16)
        for dc in (0, 1):
            cc = core if dc == 0 else 1 - core
            tp_peers.append(zz * 2 + cc)
    tp_peers.append(z * 2 + (1 - core))
    kv_peers = []
    for dist in (4, 3, 2, 1):
        for dy in (2, 1, 3, 0):
            for dx in (2, 1, 3, 0):
                if min(dy, 4 - dy) + min(dx, 4 - dx) == dist:
                    kv_peers.append(lax.rem(y + dy, 4) * 4 + lax.rem(x + dx, 4))

    barrier = pltpu.get_barrier_semaphore()
    for p in tp_peers:
        pl.semaphore_signal(barrier, inc=1, device_id={"tp": p}, device_id_type=MESH)
    for p in kv_peers:
        pl.semaphore_signal(barrier, inc=1, device_id={"kv": p}, device_id_type=MESH)

    def send(n, axis, peers, src, dst):
        for p in peers:
            pltpu.make_async_remote_copy(
                src_ref=src(p), dst_ref=dst, send_sem=ssem.at[n], recv_sem=rsem.at[n],
                device_id={axis: p}, device_id_type=MESH,
            ).start()

    def arrived(n, ref):
        pltpu.make_async_copy(ref, ref, rsem.at[n]).wait()

    def sent(n, ref):
        pltpu.make_async_copy(ref, ref, ssem.at[n]).wait()

    lane8 = iota((8, 128), 1)
    row8 = iota((8, 128), 0)
    lane1 = iota((1, 128), 1)
    ghalf8 = (lane8 // HD) == g
    mlane = (1 - g) * HD

    c_tok.wait()
    c_ag.wait()
    c_mg.wait()
    tok = tok_v[...].astype(F32)
    scaled = (tok * ag_v[...]).astype(BF16).astype(F32)
    row = jnp.concatenate(
        [scaled[0:1], scaled[1:2], scaled[2:3], tok[0:1], tok[1:2], tok[2:3], mg_v[...],
         jnp.zeros((1, 72), F32)], axis=1)
    buf1[pl.ds(tp, 1)] = row.reshape(1, 1, 128)

    wqf[pl.ds(other + 32, 32)] = jnp.zeros((32, 256), BF16)
    wo[pl.ds(other, HD)] = jnp.zeros((HD, 256), BF16)
    for w in (wg, wu, wd):
        w[FF_DEV:] = jnp.zeros((FF_PAD - FF_DEV, 256), BF16)
    c_wk.wait()
    c_wv.wait()
    wkv[...] = jnp.where(
        (iota((256, 128), 1) // HD) == g,
        wk[...].astype(F32), pltpu.roll(wv[...].astype(F32), HD, 1)).astype(BF16)
    c_wq.wait()
    c_wf.wait()

    pl.semaphore_wait(barrier, len(tp_peers) + len(kv_peers))
    send(0, "tp", tp_peers, lambda p: buf1.at[tp], buf1.at[tp])
    r24 = iota((24, 128), 0)
    b24 = r24 % 4
    want24 = jnp.where(
        r24 < 16,
        jnp.where((r24 < 4) | ((r24 >= 12) & (r24 < 16)), b24, -1),
        b24 + 3)
    l24 = iota((24, 128), 1)
    sel = jnp.where((b24 < 3) & (l24 // 8 == want24), 1.0, 0.0).astype(BF16)
    spread = (iota((256, 128), 0) % 8) == (iota((256, 128), 1) % 8)
    arrived(0, buf1.at[pl.ds(0, NTP - 1)])
    block = jnp.broadcast_to(buf1[...], (NTP, 8, 128)).reshape(256, 128)
    block = jnp.where(spread, block, 0.0)
    rows = dot(sel, block.astype(BF16), NT)
    tok_rows = rows[16:24]
    part = dot(rows[0:8].astype(BF16), wqf[...], NT) + dot(rows[8:16].astype(BF16), wkv[...], NN)
    squares = jnp.sum(tok_rows * tok_rows, axis=1, keepdims=True)
    part = jnp.where((lane8 == mlane + 32) & (row8 < 4), squares, part)
    buf2[pl.ds(kv, 1)] = part.reshape(1, 8, 128)
    send(1, "kv", kv_peers, lambda p: buf2.at[kv], buf2.at[kv])

    tok8 = jnp.where(row8 < 4, tok_rows[:, :128], tok_rows[:, 128:])
    gsel = jnp.where(lane8 // 8 == 6, 1.0, 0.0)
    gain_rows = dot(gsel, block, NT, precision=lax.Precision.HIGHEST)
    gain8 = jnp.where(row8 < 4, gain_rows[:, :128], gain_rows[:, 128:])
    c_fb.wait()
    c_og.wait()
    bias_row = jnp.concatenate([fb_v[...], jnp.zeros((1, 96), F32)], axis=1)
    bias = jnp.sum(jnp.where(lane1 == tp, bias_row, 0.0), axis=1, keepdims=True)
    og = og_v[pl.ds(z, 1)]
    og = jnp.where(core == g, og, pltpu.roll(og, HD, 1))

    arrived(1, buf2.at[pl.ds(0, NKV - 1)])
    total8 = jnp.sum(buf2[...], axis=0)
    sq = jnp.sum(jnp.where(lane8 == mlane + 32, total8, 0.0), axis=1, keepdims=True)
    rms1 = lax.rsqrt(sq * (1.0 / D) + EPS)
    q8 = jnp.where(ghalf8 & (row8 < 3), (total8 * rms1).astype(BF16).astype(F32), 0.0)
    for b in range(3):
        buf3[b, pl.ds(tp, 1)] = q8[b:b + 1].reshape(1, 1, 128)
    send(2, "tp", tp_peers, lambda p: buf3.at[:, tp], buf3.at[:, tp])

    kv8 = (pltpu.roll(total8, 4, 0) * rms1).astype(BF16).astype(F32)
    own = jnp.sum(q8 * kv8, axis=1, keepdims=True) * (HD ** -0.5)
    v8 = pltpu.roll(kv8, HD, 1)
    fj = jnp.sum(jnp.where(lane8 == mlane + tp, total8, 0.0), axis=1, keepdims=True) * rms1 + bias
    log_gate = jnp.minimum(fj, 0.0) - jnp.log1p(jnp.exp(-jnp.abs(fj)))
    c_k.wait()
    c_d.wait()
    c_v.wait()
    positions = (kv * NTP + tp) * SPAN + iota((32, SPAN), 1)
    lane32 = iota((32, 128), 1)
    ghalf32 = (lane32 // HD) == (iota((32, 128), 0) // 16)
    mlane32 = (1 - iota((32, 128), 0) // 16) * HD

    arrived(2, buf3.at[:, pl.ds(0, NTP - 1)])
    for b in range(3):
        qb = buf3[b].reshape(32, 128).astype(BF16)
        s = dot(qb, k_v[b], NN) * (HD ** -0.5) + d_v[b]
        live = positions < lengths[b]
        s = jnp.where(live, s, MASKED)
        top = jnp.max(s, axis=1, keepdims=True)
        w = jnp.where(live, jnp.exp(s - top), 0.0)
        tot = jnp.sum(w, axis=1, keepdims=True)
        vs = dot(w.astype(BF16), v_v[b], NT)
        msg = jnp.where(ghalf32, vs, jnp.where(lane32 == mlane32, top, tot))
        stage4[b] = msg.reshape(32, 1, 128)
    buf4[:, pl.ds(tp, 1)] = stage4[:, pl.ds(tp, 1)]
    send(3, "tp", tp_peers, lambda p: stage4.at[:, p], buf4.at[:, tp])

    def merge(y2):
        n = y2.shape[0]
        at_m = iota((n, 128), 1) == mlane
        m = jnp.sum(jnp.where(at_m, y2, 0.0), axis=1, keepdims=True)
        top2 = jnp.max(m, axis=0, keepdims=True)
        zsum = jnp.sum(jnp.exp(m - top2) * y2, axis=0, keepdims=True)
        return jnp.where(lane1 == mlane, top2, zsum)

    c_wo.wait()
    arrived(3, buf4.at[:, pl.ds(0, NTP - 1)])
    for b in range(3):
        buf5[b, pl.ds(kv, 1)] = merge(buf4[b].reshape(NTP, 128)).reshape(1, 1, 128)
    send(4, "kv", kv_peers, lambda p: buf5.at[:, kv], buf5.at[:, kv])
    arrived(4, buf5.at[:, pl.ds(0, NKV - 1)])
    zrow = jnp.concatenate(
        [merge(buf5[b].reshape(NKV, 128)) for b in range(3)] + [jnp.ones((5, 128), F32)], axis=0)
    m8 = jnp.sum(jnp.where(lane8 == mlane, zrow, 0.0), axis=1, keepdims=True) + log_gate
    l8 = jnp.sum(jnp.where(lane8 == mlane + 1, zrow, 0.0), axis=1, keepdims=True)
    top8 = jnp.maximum(m8, own)
    a8 = jnp.exp(m8 - top8)
    o8 = jnp.exp(own - top8)
    heads = (zrow * a8 + o8 * v8) / (l8 * a8 + o8)
    heads = jnp.where(ghalf8 & (row8 < 3), heads, 0.0)
    mean = jnp.sum(heads * heads, axis=1, keepdims=True) * (1.0 / HD)
    normed = heads * lax.rsqrt(mean + EPS) * og
    n_lo = normed.astype(BF16)
    n_hi = pltpu.roll(normed, 4, 0).astype(BF16)
    attn = dot(n_lo, wo[:, :128], NN) + dot(n_hi, wo[:, 128:], NN)
    buf6[pl.ds(tp, 1)] = attn.astype(BF16).reshape(1, 8, 128)
    send(5, "tp", tp_peers, lambda p: buf6.at[tp], buf6.at[tp])
    c_wg.wait()
    c_wu.wait()
    c_wd.wait()
    arrived(5, buf6.at[pl.ds(0, NTP - 1)])
    attn8 = jnp.sum(buf6[...].astype(F32), axis=0)
    res8 = (tok8 + attn8).astype(BF16).astype(F32)
    sc8 = (res8 * gain8).astype(BF16).astype(F32)
    sw8 = pltpu.roll(sc8, 4, 0)
    low = row8 < 4
    lhs_g = jnp.concatenate([jnp.where(low, sc8, 0.0), jnp.where(low, sw8, 0.0)], axis=1).astype(BF16)
    lhs_u = jnp.concatenate([jnp.where(low, 0.0, sw8), jnp.where(low, 0.0, sc8)], axis=1).astype(BF16)
    gu = dot(lhs_g, wg[...], NT) + dot(lhs_u, wu[...], NT)
    sq2 = jnp.sum(res8 * res8, axis=1, keepdims=True) + jnp.zeros((8, 128), F32)
    sq2 = sq2 + pltpu.roll(sq2, 4, 0)
    sq2_hi = sq2.astype(BF16).astype(F32)
    lane_t = lane8 + 256
    tail = jnp.where(lane_t == FF_DEV, sq2_hi, jnp.where(lane_t == FF_DEV + 1, sq2 - sq2_hi, gu[:, 256:]))
    gu = jnp.concatenate([gu[:, :256], tail], axis=1)
    buf7[pl.ds(kv, 1)] = gu.astype(BF16).reshape(1, 8, FF_PAD)
    send(6, "kv", kv_peers, lambda p: buf7.at[kv], buf7.at[kv])

    i64 = iota((64, 256), 0)
    n64 = iota((64, 256), 1)
    res_rows = jnp.concatenate([res8, pltpu.roll(res8, 4, 0)], axis=1)
    rep = jnp.broadcast_to(res_rows.reshape(8, 1, 256), (8, 8, 256)).reshape(64, 256)
    diag = (i64 % 8) == (n64 % 8)
    mine = jnp.where(iota((8, 256), 1) // 8 == tp, 1.0, 0.0).astype(BF16)
    res_mine = dot(mine, jnp.where(diag, rep, 0.0).astype(BF16), NT)[0:1]
    fold = jnp.where(iota((32, 256), 1) // 8 == iota((32, 256), 0), 1.0, 0.0).astype(BF16)

    arrived(6, buf7.at[pl.ds(0, NKV - 1)])
    gs = jnp.sum(buf7[...].astype(F32), axis=0)
    tail = gs[:, 256:]
    sq2 = jnp.sum(
        jnp.where((lane_t == FF_DEV) | (lane_t == FF_DEV + 1), tail, 0.0), axis=1, keepdims=True)
    rms2 = lax.rsqrt(sq2 * (1.0 / D) + EPS)
    gs = gs * jnp.concatenate([rms2[0:4], rms2[0:4]], axis=0)
    up = pltpu.roll(gs, 4, 0)
    hid = gs / (1.0 + jnp.exp(-gs)) * up
    hid = jnp.where((iota((8, FF_PAD), 1) < FF_DEV) & (iota((8, FF_PAD), 0) < 3), hid, 0.0)
    hid = jnp.broadcast_to(hid.reshape(8, 1, FF_PAD), (8, 8, FF_PAD)).reshape(64, FF_PAD)
    down = dot(hid.astype(BF16), wd[...], NN)
    down = jnp.where(diag, down, 0.0)
    d_hi = down.astype(BF16)
    d_lo = (down - d_hi.astype(F32)).astype(BF16)
    parts = dot(fold, d_hi, NT) + dot(fold, d_lo, NT)
    parts = jnp.concatenate([parts, jnp.zeros((32, 64), F32)], axis=1)
    stage8[...] = parts.reshape(32, 1, 128)
    buf8[pl.ds(tp, 1)] = stage8[pl.ds(tp, 1)]
    send(7, "tp", tp_peers, lambda p: stage8.at[p], buf8.at[tp])
    arrived(7, buf8.at[pl.ds(0, NTP - 1)])
    share = jnp.sum(buf8[...], axis=0)[:, :64] + res_mine
    out[...] = jnp.concatenate([share[:, 0:8], share[:, 8:16], share[:, 16:24]], axis=0).astype(BF16)

    sent(0, buf1.at[pl.ds(0, NTP - 1)])
    sent(1, buf2.at[pl.ds(0, NKV - 1)])
    sent(2, buf3.at[:, pl.ds(0, NTP - 1)])
    sent(3, buf4.at[:, pl.ds(0, NTP - 1)])
    sent(4, buf5.at[:, pl.ds(0, NKV - 1)])
    sent(5, buf6.at[pl.ds(0, NTP - 1)])
    sent(6, buf7.at[pl.ds(0, NKV - 1)])
    sent(7, buf8.at[pl.ds(0, NTP - 1)])


def body(
    tokens, lengths, attn_gain, w_query, w_key, w_value, w_forget, forget_bias,
    cache_keys, cache_values, cache_decay, out_gain, w_out, mlp_gain, w_gate, w_up, w_down,
):
    hbm = pl.BlockSpec(memory_space=pl.ANY)
    v = pltpu.VMEM
    return pl.pallas_call(
        kernel,
        out_shape=pltpu.VMEM((3, 8), BF16),
        in_specs=[pl.BlockSpec(memory_space=pltpu.SMEM)] + [hbm] * 16,
        out_specs=pl.BlockSpec(memory_space=pltpu.VMEM),
        scratch_shapes=[
            v((3, 8), BF16), v((1, 8), F32), v((1, 8), F32), v((1, 32), F32), v((16, 128), F32),
            v((128, 256), BF16), v((256, 128), BF16), v((256, 128), BF16), v((256, 128), BF16),
            v((3, 128, SPAN), BF16), v((3, 128, SPAN), BF16), v((3, 32, SPAN), F32),
            v((128, 256), BF16),
            v((FF_PAD, 256), BF16), v((FF_PAD, 256), BF16), v((FF_PAD, 256), BF16),
            v((NTP, 1, 128), F32), v((NKV, 8, 128), F32), v((3, NTP, 1, 128), F32),
            v((3, NTP, 1, 128), F32), v((3, NTP, 1, 128), F32), v((3, NKV, 1, 128), F32),
            v((NTP, 8, 128), BF16), v((NKV, 8, FF_PAD), BF16),
            v((NTP, 1, 128), F32), v((NTP, 1, 128), F32),
            pltpu.SemaphoreType.DMA((16,)),
            pltpu.SemaphoreType.DMA((8,)),
            pltpu.SemaphoreType.DMA((8,)),
        ],
        compiler_params=pltpu.CompilerParams(
            collective_id=0, has_side_effects=True, vmem_limit_bytes=60 * 1024 * 1024),
    )(
        lengths, tokens, attn_gain.reshape(1, 8), mlp_gain.reshape(1, 8),
        forget_bias.reshape(1, 32), out_gain.reshape(16, 128),
        w_query.T, w_key, w_value, w_forget.T, cache_keys, cache_values, cache_decay, w_out,
        w_gate.T, w_up.T, w_down,
    )


def solution(mesh):
    kvtp = ("kv", "tp")
    placed = (
        P(None, kvtp), P(), P(kvtp), P("kv", "tp"), P("kv", None), P("kv", None), P(), P(),
        P(None, None, kvtp), P(None, None, kvtp), P(None, None, kvtp), P(), P("tp", "kv"),
        P(kvtp), P("kv", "tp"), P("kv", "tp"), P("tp", "kv"),
    )
    return jax.shard_map(
        body, mesh=mesh, in_specs=placed, out_specs=P(None, kvtp), check_vma=False)
```

```python
import jax
import jax.numpy as jnp
from jax import lax
from jax.experimental import pallas as pl
from jax.experimental.pallas import tpu as pltpu
from jax.sharding import PartitionSpec as P

MESH = pl.DeviceIdType.MESH
D = 4096
HD = 64
NTP = 32
NKV = 16
FF_DEV = 352
FF_PAD = 384
SPAN = 256
EPS = 1e-06
MASKED = -1e30
F32 = jnp.float32
BF16 = jnp.bfloat16

NT = (((1,), (1,)), ((), ()))
NN = (((1,), (0,)), ((), ()))

def dot(a, b, dims, **kw):
    return lax.dot_general(a, b, dims, preferred_element_type=F32, **kw)


def iota(shape, dim):
    return lax.broadcasted_iota(jnp.int32, shape, dim)


def kernel(
    lengths_h, tokens, attn_gain, mlp_gain, forget_bias, out_gain,
    w_query, w_key, w_value, w_forget, keys, values, decay, w_out,
    w_gate, w_up, w_down,
    out,
    lengths, tok_v, ag_v, mg_v, fb_v, og_v, wqf, wk, wv, wkv, k_v, v_v, d_v, wo,
    wg, wu, wd,
    buf1, buf2, buf3, stage4, buf4, buf5, buf6, buf7, stage8, buf8,
    lsem, ssem, rsem,
):
    kv = lax.axis_index("kv")
    tp = lax.axis_index("tp")
    g = tp // 16
    z = tp // 2
    core = tp % 2
    y = kv // 4
    x = kv % 4

    kv_peers = []
    for dist in (4, 3, 2, 1):
        for dy in (2, 1, 3, 0):
            for dx in (2, 1, 3, 0):
                if min(dy, 4 - dy) + min(dx, 4 - dx) == dist:
                    kv_peers.append(lax.rem(y + dy, 4) * 4 + lax.rem(x + dx, 4))

    barrier = pltpu.get_barrier_semaphore()

    def far_peer(i):
        s = i // 2
        d = 8 - (s + 1) // 2
        return lax.rem(z + d + (16 - 2 * d) * (1 - s % 2), 16) * 2 + lax.rem(core + i, 2)

    def greet(i, carry):
        pl.semaphore_signal(barrier, inc=1, device_id={"tp": far_peer(i)}, device_id_type=MESH)
        return carry
    lax.fori_loop(0, 30, greet, 0)
    partner = z * 2 + (1 - core)
    pl.semaphore_signal(barrier, inc=1, device_id={"tp": partner}, device_id_type=MESH)
    for p in kv_peers:
        pl.semaphore_signal(barrier, inc=1, device_id={"kv": p}, device_id_type=MESH)

    def load(i, src, dst):
        c = pltpu.make_async_copy(src, dst, lsem.at[i])
        c.start()
        return c

    half = pl.multiple_of(g * HD, HD)
    other = pl.multiple_of((1 - g) * HD, HD)
    c_tok = load(0, tokens, tok_v)
    c_ag = load(1, attn_gain, ag_v)
    c_mg = load(2, mlp_gain, mg_v)
    c_wq = load(3, w_query, wqf.at[pl.ds(half, HD)])
    cols = pl.ds(pl.multiple_of(kv * 256, 256), 256)
    c_wf = load(4, w_forget.at[:, cols], wqf.at[pl.ds(other, 32)])
    c_wk = load(5, w_key, wk)
    c_wv = load(6, w_value, wv)
    c_k = load(7, keys, k_v)
    c_d = load(8, decay, d_v)
    c_v = load(9, values, v_v)
    c_fb = load(10, forget_bias, fb_v)
    c_og = load(11, out_gain, og_v)
    c_wo = load(12, w_out, wo.at[pl.ds(half, HD)])
    c_wg = load(13, w_gate, wg.at[pl.ds(0, FF_DEV)])
    c_wu = load(14, w_up, wu.at[pl.ds(0, FF_DEV)])
    c_wd = load(15, w_down, wd.at[pl.ds(0, FF_DEV)])
    c_len = load(16, lengths_h, lengths)

    def send(n, axis, peers, src, dst):
        def one(p):
            pltpu.make_async_remote_copy(
                src_ref=src(p), dst_ref=dst, send_sem=ssem.at[n], recv_sem=rsem.at[n],
                device_id={axis: p}, device_id_type=MESH,
            ).start()
        if axis == "kv":
            for p in peers:
                one(p)
            return

        def step(i, carry):
            one(far_peer(i))
            return carry
        lax.fori_loop(0, 30, step, 0)
        one(partner)

    def arrived(n, ref):
        pltpu.make_async_copy(ref, ref, rsem.at[n]).wait()

    def sent(n, ref):
        pltpu.make_async_copy(ref, ref, ssem.at[n]).wait()

    lane8 = iota((8, 128), 1)
    row8 = iota((8, 128), 0)
    lane1 = iota((1, 128), 1)
    ghalf8 = (lane8 // HD) == g
    mlane = (1 - g) * HD

    c_tok.wait()
    c_ag.wait()
    c_mg.wait()
    tok = tok_v[...].astype(F32)
    scaled = (tok * ag_v[...]).astype(BF16).astype(F32)
    row = jnp.concatenate(
        [scaled[0:1], scaled[1:2], scaled[2:3], tok[0:1], tok[1:2], tok[2:3], mg_v[...],
         jnp.zeros((1, 72), F32)], axis=1)
    buf1[pl.ds(tp, 1)] = row.reshape(1, 1, 128)

    wqf[pl.ds(other + 32, 32)] = jnp.zeros((32, 256), BF16)
    wo[pl.ds(other, HD)] = jnp.zeros((HD, 256), BF16)
    for w in (wg, wu, wd):
        w[FF_DEV:] = jnp.zeros((FF_PAD - FF_DEV, 256), BF16)
    c_wk.wait()
    c_wv.wait()
    wkv[...] = jnp.where(
        (iota((256, 128), 1) // HD) == g,
        wk[...].astype(F32), pltpu.roll(wv[...].astype(F32), HD, 1)).astype(BF16)
    c_wq.wait()
    c_wf.wait()

    pl.semaphore_wait(barrier, NTP - 1 + len(kv_peers))
    send(0, "tp", (), lambda p: buf1.at[tp], buf1.at[tp])
    r24 = iota((24, 128), 0)
    b24 = r24 % 4
    want24 = jnp.where(
        r24 < 16,
        jnp.where((r24 < 4) | ((r24 >= 12) & (r24 < 16)), b24, -1),
        b24 + 3)
    l24 = iota((24, 128), 1)
    sel = jnp.where((b24 < 3) & (l24 // 8 == want24), 1.0, 0.0).astype(BF16)
    spread = (iota((256, 128), 0) % 8) == (iota((256, 128), 1) % 8)
    arrived(0, buf1.at[pl.ds(0, NTP - 1)])
    block = jnp.broadcast_to(buf1[...], (NTP, 8, 128)).reshape(256, 128)
    block = jnp.where(spread, block, 0.0)
    rows = dot(sel, block.astype(BF16), NT)
    tok_rows = rows[16:24]
    part = dot(rows[0:8].astype(BF16), wqf[...], NT) + dot(rows[8:16].astype(BF16), wkv[...], NN)
    squares = jnp.sum(tok_rows * tok_rows, axis=1, keepdims=True)
    part = jnp.where((lane8 == mlane + 32) & (row8 < 4), squares, part)
    buf2[pl.ds(kv, 1)] = part.reshape(1, 8, 128)
    send(1, "kv", kv_peers, lambda p: buf2.at[kv], buf2.at[kv])

    tok8 = jnp.where(row8 < 4, tok_rows[:, :128], tok_rows[:, 128:])
    gsel = jnp.where(lane8 // 8 == 6, 1.0, 0.0)
    gain_rows = dot(gsel, block, NT, precision=lax.Precision.HIGHEST)
    gain8 = jnp.where(row8 < 4, gain_rows[:, :128], gain_rows[:, 128:])
    c_fb.wait()
    c_og.wait()
    bias_row = jnp.concatenate([fb_v[...], jnp.zeros((1, 96), F32)], axis=1)
    bias = jnp.sum(jnp.where(lane1 == tp, bias_row, 0.0), axis=1, keepdims=True)
    og = og_v[pl.ds(z, 1)]
    og = jnp.where(core == g, og, pltpu.roll(og, HD, 1))

    sent(0, buf1.at[pl.ds(0, NTP - 1)])
    arrived(1, buf2.at[pl.ds(0, NKV - 1)])
    total8 = jnp.sum(buf2[...], axis=0)
    sq = jnp.sum(jnp.where(lane8 == mlane + 32, total8, 0.0), axis=1, keepdims=True)
    rms1 = lax.rsqrt(sq * (1.0 / D) + EPS)
    q8 = jnp.where(ghalf8 & (row8 < 3), (total8 * rms1).astype(BF16).astype(F32), 0.0)
    for b in range(3):
        buf3[b, pl.ds(tp, 1)] = q8[b:b + 1].reshape(1, 1, 128)
    send(2, "tp", (), lambda p: buf3.at[:, tp], buf3.at[:, tp])

    kv8 = (pltpu.roll(total8, 4, 0) * rms1).astype(BF16).astype(F32)
    own = jnp.sum(q8 * kv8, axis=1, keepdims=True) * (HD ** -0.5)
    v8 = pltpu.roll(kv8, HD, 1)
    fj = jnp.sum(jnp.where(lane8 == mlane + tp, total8, 0.0), axis=1, keepdims=True) * rms1 + bias
    log_gate = jnp.minimum(fj, 0.0) - jnp.log1p(jnp.exp(-jnp.abs(fj)))
    c_k.wait()
    c_d.wait()
    c_v.wait()
    c_len.wait()
    positions = (kv * NTP + tp) * SPAN + iota((32, SPAN), 1)
    lane32 = iota((32, 128), 1)
    ghalf32 = (lane32 // HD) == (iota((32, 128), 0) // 16)
    mlane32 = (1 - iota((32, 128), 0) // 16) * HD

    sent(1, buf2.at[pl.ds(0, NKV - 1)])
    arrived(2, buf3.at[:, pl.ds(0, NTP - 1)])
    for b in range(3):
        qb = buf3[b].reshape(32, 128).astype(BF16)
        s = dot(qb, k_v[b], NN) * (HD ** -0.5) + d_v[b]
        live = positions < lengths[b]
        s = jnp.where(live, s, MASKED)
        top = jnp.max(s, axis=1, keepdims=True)
        w = jnp.where(live, jnp.exp(s - top), 0.0)
        tot = jnp.sum(w, axis=1, keepdims=True)
        vs = dot(w.astype(BF16), v_v[b], NT)
        msg = jnp.where(ghalf32, vs, jnp.where(lane32 == mlane32, top, tot))
        stage4[b] = msg.reshape(32, 1, 128)
    buf4[:, pl.ds(tp, 1)] = stage4[:, pl.ds(tp, 1)]
    send(3, "tp", (), lambda p: stage4.at[:, p], buf4.at[:, tp])

    def merge(y2):
        n = y2.shape[0]
        at_m = iota((n, 128), 1) == mlane
        m = jnp.sum(jnp.where(at_m, y2, 0.0), axis=1, keepdims=True)
        top2 = jnp.max(m, axis=0, keepdims=True)
        zsum = jnp.sum(jnp.exp(m - top2) * y2, axis=0, keepdims=True)
        return jnp.where(lane1 == mlane, top2, zsum)

    c_wo.wait()
    sent(2, buf3.at[:, pl.ds(0, NTP - 1)])
    arrived(3, buf4.at[:, pl.ds(0, NTP - 1)])
    for b in range(3):
        buf5[b, pl.ds(kv, 1)] = merge(buf4[b].reshape(NTP, 128)).reshape(1, 1, 128)
    send(4, "kv", kv_peers, lambda p: buf5.at[:, kv], buf5.at[:, kv])
    sent(3, buf4.at[:, pl.ds(0, NTP - 1)])
    arrived(4, buf5.at[:, pl.ds(0, NKV - 1)])
    zrow = jnp.concatenate(
        [merge(buf5[b].reshape(NKV, 128)) for b in range(3)] + [jnp.ones((5, 128), F32)], axis=0)
    m8 = jnp.sum(jnp.where(lane8 == mlane, zrow, 0.0), axis=1, keepdims=True) + log_gate
    l8 = jnp.sum(jnp.where(lane8 == mlane + 1, zrow, 0.0), axis=1, keepdims=True)
    top8 = jnp.maximum(m8, own)
    a8 = jnp.exp(m8 - top8)
    o8 = jnp.exp(own - top8)
    heads = (zrow * a8 + o8 * v8) / (l8 * a8 + o8)
    heads = jnp.where(ghalf8 & (row8 < 3), heads, 0.0)
    mean = jnp.sum(heads * heads, axis=1, keepdims=True) * (1.0 / HD)
    normed = heads * lax.rsqrt(mean + EPS) * og
    n_lo = normed.astype(BF16)
    n_hi = pltpu.roll(normed, 4, 0).astype(BF16)
    attn = dot(n_lo, wo[:, :128], NN) + dot(n_hi, wo[:, 128:], NN)
    buf6[pl.ds(tp, 1)] = attn.astype(BF16).reshape(1, 8, 128)
    send(5, "tp", (), lambda p: buf6.at[tp], buf6.at[tp])
    c_wg.wait()
    c_wu.wait()
    c_wd.wait()
    sent(4, buf5.at[:, pl.ds(0, NKV - 1)])
    arrived(5, buf6.at[pl.ds(0, NTP - 1)])
    attn8 = jnp.sum(buf6[...].astype(F32), axis=0)
    res8 = (tok8 + attn8).astype(BF16).astype(F32)
    sc8 = (res8 * gain8).astype(BF16).astype(F32)
    sw8 = pltpu.roll(sc8, 4, 0)
    low = row8 < 4
    lhs_g = jnp.concatenate([jnp.where(low, sc8, 0.0), jnp.where(low, sw8, 0.0)], axis=1).astype(BF16)
    lhs_u = jnp.concatenate([jnp.where(low, 0.0, sw8), jnp.where(low, 0.0, sc8)], axis=1).astype(BF16)
    gu = dot(lhs_g, wg[...], NT) + dot(lhs_u, wu[...], NT)
    sq2 = jnp.sum(res8 * res8, axis=1, keepdims=True) + jnp.zeros((8, 128), F32)
    sq2 = sq2 + pltpu.roll(sq2, 4, 0)
    sq2_hi = sq2.astype(BF16).astype(F32)
    lane_t = lane8 + 256
    tail = jnp.where(lane_t == FF_DEV, sq2_hi, jnp.where(lane_t == FF_DEV + 1, sq2 - sq2_hi, gu[:, 256:]))
    gu = jnp.concatenate([gu[:, :256], tail], axis=1)
    buf7[pl.ds(kv, 1)] = gu.astype(BF16).reshape(1, 8, FF_PAD)
    send(6, "kv", kv_peers, lambda p: buf7.at[kv], buf7.at[kv])

    i64 = iota((64, 256), 0)
    n64 = iota((64, 256), 1)
    res_rows = jnp.concatenate([res8, pltpu.roll(res8, 4, 0)], axis=1)
    rep = jnp.broadcast_to(res_rows.reshape(8, 1, 256), (8, 8, 256)).reshape(64, 256)
    diag = (i64 % 8) == (n64 % 8)
    mine = jnp.where(iota((8, 256), 1) // 8 == tp, 1.0, 0.0).astype(BF16)
    res_mine = dot(mine, jnp.where(diag, rep, 0.0).astype(BF16), NT)[0:1]
    fold = jnp.where(iota((32, 256), 1) // 8 == iota((32, 256), 0), 1.0, 0.0).astype(BF16)

    sent(5, buf6.at[pl.ds(0, NTP - 1)])
    arrived(6, buf7.at[pl.ds(0, NKV - 1)])
    gs = jnp.sum(buf7[...].astype(F32), axis=0)
    tail = gs[:, 256:]
    sq2 = jnp.sum(
        jnp.where((lane_t == FF_DEV) | (lane_t == FF_DEV + 1), tail, 0.0), axis=1, keepdims=True)
    rms2 = lax.rsqrt(sq2 * (1.0 / D) + EPS)
    gs = gs * jnp.concatenate([rms2[0:4], rms2[0:4]], axis=0)
    up = pltpu.roll(gs, 4, 0)
    hid = gs / (1.0 + jnp.exp(-gs)) * up
    hid = jnp.where((iota((8, FF_PAD), 1) < FF_DEV) & (iota((8, FF_PAD), 0) < 3), hid, 0.0)
    hid = jnp.broadcast_to(hid.reshape(8, 1, FF_PAD), (8, 8, FF_PAD)).reshape(64, FF_PAD)
    down = dot(hid.astype(BF16), wd[...], NN)
    down = jnp.where(diag, down, 0.0)
    d_hi = down.astype(BF16)
    d_lo = (down - d_hi.astype(F32)).astype(BF16)
    parts = dot(fold, d_hi, NT) + dot(fold, d_lo, NT)
    parts = jnp.concatenate([parts, jnp.zeros((32, 64), F32)], axis=1)
    stage8[...] = parts.reshape(32, 1, 128)
    buf8[pl.ds(tp, 1)] = stage8[pl.ds(tp, 1)]
    send(7, "tp", (), lambda p: stage8.at[p], buf8.at[tp])
    sent(6, buf7.at[pl.ds(0, NKV - 1)])
    arrived(7, buf8.at[pl.ds(0, NTP - 1)])
    share = jnp.sum(buf8[...], axis=0)[:, :64] + res_mine
    out[...] = jnp.concatenate([share[:, 0:8], share[:, 8:16], share[:, 16:24]], axis=0).astype(BF16)
    sent(7, buf8.at[pl.ds(0, NTP - 1)])


def body(
    tokens, lengths, attn_gain, w_query, w_key, w_value, w_forget, forget_bias,
    cache_keys, cache_values, cache_decay, out_gain, w_out, mlp_gain, w_gate, w_up, w_down,
):
    hbm = pl.BlockSpec(memory_space=pl.ANY)
    v = pltpu.VMEM
    return pl.pallas_call(
        kernel,
        out_shape=pltpu.VMEM((3, 8), BF16),
        in_specs=[hbm] * 17,
        out_specs=pl.BlockSpec(memory_space=pltpu.VMEM),
        scratch_shapes=[
            pltpu.SMEM((3,), jnp.int32), v((3, 8), BF16), v((1, 8), F32), v((1, 8), F32), v((1, 32), F32), v((16, 128), F32),
            v((128, 256), BF16), v((256, 128), BF16), v((256, 128), BF16), v((256, 128), BF16),
            v((3, 128, SPAN), BF16), v((3, 128, SPAN), BF16), v((3, 32, SPAN), F32),
            v((128, 256), BF16),
            v((FF_PAD, 256), BF16), v((FF_PAD, 256), BF16), v((FF_PAD, 256), BF16),
            v((NTP, 1, 128), F32), v((NKV, 8, 128), F32), v((3, NTP, 1, 128), F32),
            v((3, NTP, 1, 128), F32), v((3, NTP, 1, 128), F32), v((3, NKV, 1, 128), F32),
            v((NTP, 8, 128), BF16), v((NKV, 8, FF_PAD), BF16),
            v((NTP, 1, 128), F32), v((NTP, 1, 128), F32),
            pltpu.SemaphoreType.DMA((17,)),
            pltpu.SemaphoreType.DMA((8,)),
            pltpu.SemaphoreType.DMA((8,)),
        ],
        compiler_params=pltpu.CompilerParams(
            collective_id=0, has_side_effects=True, vmem_limit_bytes=60 * 1024 * 1024),
    )(
        lengths, tokens, attn_gain.reshape(1, 8), mlp_gain.reshape(1, 8),
        forget_bias.reshape(1, 32), out_gain.reshape(16, 128),
        w_query.T, w_key, w_value, w_forget.T, cache_keys, cache_values, cache_decay, w_out,
        w_gate.T, w_up.T, w_down,
    )


def solution(mesh):
    kvtp = ("kv", "tp")
    placed = (
        P(None, kvtp), P(), P(kvtp), P("kv", "tp"), P("kv", None), P("kv", None), P(), P(),
        P(None, None, kvtp), P(None, None, kvtp), P(None, None, kvtp), P(), P("tp", "kv"),
        P(kvtp), P("kv", "tp"), P("kv", "tp"), P("tp", "kv"),
    )
    return jax.shard_map(
        body, mesh=mesh, in_specs=placed, out_specs=P(None, kvtp), check_vma=False)
```

```python
import jax
import jax.numpy as jnp
from jax import lax
from jax.experimental import pallas as pl
from jax.experimental.pallas import tpu as pltpu
from jax.sharding import PartitionSpec as P

MESH = pl.DeviceIdType.MESH
D = 4096
HD = 64
NTP = 32
NKV = 16
FF_DEV = 352
FF_PAD = 384
SPAN = 256
EPS = 1e-06
MASKED = -1e30
F32 = jnp.float32
BF16 = jnp.bfloat16

NT = (((1,), (1,)), ((), ()))
NN = (((1,), (0,)), ((), ()))

def dot(a, b, dims, **kw):
    return lax.dot_general(a, b, dims, preferred_element_type=F32, **kw)


def iota(shape, dim):
    return lax.broadcasted_iota(jnp.int32, shape, dim)


def kernel(
    lengths_h, tokens, attn_gain, mlp_gain, forget_bias, out_gain,
    w_query, w_key, w_value, w_forget, keys, values, decay, w_out,
    w_gate, w_up, w_down,
    out,
    lengths, tok_v, ag_v, mg_v, fb_v, og_v, wqf, wk, wv, wkv, k_v, v_v, d_v, wo,
    wg, wu, wd,
    buf1, buf2, buf3, stage4, buf4, buf5, buf6, buf7, stage8, buf8,
    lsem, ssem, rsem, pair_ready,
):
    kv = lax.axis_index("kv")
    tp = lax.axis_index("tp")
    g = tp // 16
    z = tp // 2
    core = tp % 2
    y = kv // 4
    x = kv % 4

    kv_peers = []
    for dist in (4, 3, 2, 1):
        for dy in (2, 1, 3, 0):
            for dx in (2, 1, 3, 0):
                if min(dy, 4 - dy) + min(dx, 4 - dx) == dist:
                    kv_peers.append(lax.rem(y + dy, 4) * 4 + lax.rem(x + dx, 4))

    barrier = pltpu.get_barrier_semaphore()

    def far_peer(i):
        s = i // 2
        d = 8 - (s + 1) // 2
        return lax.rem(z + d + (16 - 2 * d) * (1 - s % 2), 16) * 2 + lax.rem(core + i, 2)

    def greet(s, carry):
        pl.semaphore_signal(barrier, inc=1, device_id={"tp": far_peer(2 * s)}, device_id_type=MESH)
        return carry
    lax.fori_loop(0, 15, greet, 0)
    partner = z * 2 + (1 - core)
    pl.semaphore_signal(barrier, inc=1, device_id={"tp": partner}, device_id_type=MESH)
    for p in kv_peers:
        pl.semaphore_signal(barrier, inc=1, device_id={"kv": p}, device_id_type=MESH)

    def load(i, src, dst):
        c = pltpu.make_async_copy(src, dst, lsem.at[i])
        c.start()
        return c

    half = pl.multiple_of(g * HD, HD)
    other = pl.multiple_of((1 - g) * HD, HD)
    c_tok = load(0, tokens, tok_v)
    c_ag = load(1, attn_gain, ag_v)
    c_mg = load(2, mlp_gain, mg_v)
    c_wq = load(3, w_query, wqf.at[pl.ds(half, HD)])
    cols = pl.ds(pl.multiple_of(kv * 256, 256), 256)
    c_wf = load(4, w_forget.at[:, cols], wqf.at[pl.ds(other, 32)])
    c_wk = load(5, w_key, wk)
    c_wv = load(6, w_value, wv)
    c_k = load(7, keys, k_v)
    c_d = load(8, decay, d_v)
    c_v = load(9, values, v_v)
    c_fb = load(10, forget_bias, fb_v)
    c_og = load(11, out_gain, og_v)
    c_wo = load(12, w_out, wo.at[pl.ds(half, HD)])
    c_wg = load(13, w_gate, wg.at[pl.ds(0, FF_DEV)])
    c_wu = load(14, w_up, wu.at[pl.ds(0, FF_DEV)])
    c_wd = load(15, w_down, wd.at[pl.ds(0, FF_DEV)])
    c_len = load(16, lengths_h, lengths)

    def send(n, axis, peers, src, dst):
        def one(p):
            pltpu.make_async_remote_copy(
                src_ref=src(p), dst_ref=dst, send_sem=ssem.at[n], recv_sem=rsem.at[n],
                device_id={axis: p}, device_id_type=MESH,
            ).start()
        if axis == "kv":
            for p in peers:
                one(p)
            return

        def step(i, carry):
            one(far_peer(i))
            return carry
        lax.fori_loop(0, 30, step, 0)
        one(partner)

    def arrived(n, ref):
        pltpu.make_async_copy(ref, ref, rsem.at[n]).wait()

    def sent(n, ref):
        pltpu.make_async_copy(ref, ref, ssem.at[n]).wait()

    lane8 = iota((8, 128), 1)
    row8 = iota((8, 128), 0)
    lane1 = iota((1, 128), 1)
    ghalf8 = (lane8 // HD) == g
    mlane = (1 - g) * HD

    c_tok.wait()
    c_ag.wait()
    c_mg.wait()
    tok = tok_v[...].astype(F32)
    scaled = (tok * ag_v[...]).astype(BF16).astype(F32)
    row = jnp.concatenate(
        [scaled[0:1], scaled[1:2], scaled[2:3], tok[0:1], tok[1:2], tok[2:3], mg_v[...],
         jnp.zeros((1, 72), F32)], axis=1)
    buf1[pl.ds(tp, 1)] = row.reshape(1, 1, 128)

    wqf[pl.ds(other + 32, 32)] = jnp.zeros((32, 256), BF16)
    wo[pl.ds(other, HD)] = jnp.zeros((HD, 256), BF16)
    for w in (wg, wu, wd):
        w[FF_DEV:] = jnp.zeros((FF_PAD - FF_DEV, 256), BF16)
    c_wk.wait()
    c_wv.wait()
    wkv[...] = jnp.where(
        (iota((256, 128), 1) // HD) == g,
        wk[...].astype(F32), pltpu.roll(wv[...].astype(F32), HD, 1)).astype(BF16)
    c_wq.wait()
    c_wf.wait()

    pl.semaphore_wait(barrier, 16 + len(kv_peers))
    pl.semaphore_signal(pair_ready, inc=1, device_id={"tp": partner}, device_id_type=MESH)

    def token_copy(p):
        pltpu.make_async_remote_copy(
            src_ref=buf1.at[tp], dst_ref=buf1.at[tp], send_sem=ssem.at[0], recv_sem=rsem.at[0],
            device_id={"tp": p}, device_id_type=MESH,
        ).start()

    def same_core(s, carry):
        token_copy(far_peer(2 * s))
        return carry

    def other_core(s, carry):
        token_copy(far_peer(2 * s + 1))
        return carry
    lax.fori_loop(0, 15, same_core, 0)
    pl.semaphore_wait(pair_ready, 1)
    lax.fori_loop(0, 15, other_core, 0)
    token_copy(partner)
    r24 = iota((24, 128), 0)
    b24 = r24 % 4
    want24 = jnp.where(
        r24 < 16,
        jnp.where((r24 < 4) | ((r24 >= 12) & (r24 < 16)), b24, -1),
        b24 + 3)
    l24 = iota((24, 128), 1)
    sel = jnp.where((b24 < 3) & (l24 // 8 == want24), 1.0, 0.0).astype(BF16)
    spread = (iota((256, 128), 0) % 8) == (iota((256, 128), 1) % 8)
    arrived(0, buf1.at[pl.ds(0, NTP - 1)])
    block = jnp.broadcast_to(buf1[...], (NTP, 8, 128)).reshape(256, 128)
    block = jnp.where(spread, block, 0.0)
    rows = dot(sel, block.astype(BF16), NT)
    tok_rows = rows[16:24]
    part = dot(rows[0:8].astype(BF16), wqf[...], NT) + dot(rows[8:16].astype(BF16), wkv[...], NN)
    squares = jnp.sum(tok_rows * tok_rows, axis=1, keepdims=True)
    part = jnp.where((lane8 == mlane + 32) & (row8 < 4), squares, part)
    buf2[pl.ds(kv, 1)] = part.reshape(1, 8, 128)
    send(1, "kv", kv_peers, lambda p: buf2.at[kv], buf2.at[kv])

    tok8 = jnp.where(row8 < 4, tok_rows[:, :128], tok_rows[:, 128:])
    gsel = jnp.where(lane8 // 8 == 6, 1.0, 0.0)
    gain_rows = dot(gsel, block, NT, precision=lax.Precision.HIGHEST)
    gain8 = jnp.where(row8 < 4, gain_rows[:, :128], gain_rows[:, 128:])
    c_fb.wait()
    c_og.wait()
    bias_row = jnp.concatenate([fb_v[...], jnp.zeros((1, 96), F32)], axis=1)
    bias = jnp.sum(jnp.where(lane1 == tp, bias_row, 0.0), axis=1, keepdims=True)
    og = og_v[pl.ds(z, 1)]
    og = jnp.where(core == g, og, pltpu.roll(og, HD, 1))

    sent(0, buf1.at[pl.ds(0, NTP - 1)])
    arrived(1, buf2.at[pl.ds(0, NKV - 1)])
    total8 = jnp.sum(buf2[...], axis=0)
    sq = jnp.sum(jnp.where(lane8 == mlane + 32, total8, 0.0), axis=1, keepdims=True)
    rms1 = lax.rsqrt(sq * (1.0 / D) + EPS)
    q8 = jnp.where(ghalf8 & (row8 < 3), (total8 * rms1).astype(BF16).astype(F32), 0.0)
    for b in range(3):
        buf3[b, pl.ds(tp, 1)] = q8[b:b + 1]
    send(2, "tp", (), lambda p: buf3.at[:, pl.ds(tp, 1)], buf3.at[:, pl.ds(tp, 1)])

    kv8 = (pltpu.roll(total8, 4, 0) * rms1).astype(BF16).astype(F32)
    own = jnp.sum(q8 * kv8, axis=1, keepdims=True) * (HD ** -0.5)
    v8 = pltpu.roll(kv8, HD, 1)
    fj = jnp.sum(jnp.where(lane8 == mlane + tp, total8, 0.0), axis=1, keepdims=True) * rms1 + bias
    log_gate = jnp.minimum(fj, 0.0) - jnp.log1p(jnp.exp(-jnp.abs(fj)))
    c_k.wait()
    c_d.wait()
    c_v.wait()
    c_len.wait()
    positions = (kv * NTP + tp) * SPAN + iota((32, SPAN), 1)
    lane32 = iota((32, 128), 1)
    ghalf32 = (lane32 // HD) == (iota((32, 128), 0) // 16)
    mlane32 = (1 - iota((32, 128), 0) // 16) * HD

    sent(1, buf2.at[pl.ds(0, NKV - 1)])
    arrived(2, buf3.at[:, pl.ds(0, NTP - 1)])
    for b in range(3):
        qb = buf3[b].astype(BF16)
        s = dot(qb, k_v[b], NN) * (HD ** -0.5) + d_v[b]
        live = positions < lengths[b]
        s = jnp.where(live, s, MASKED)
        top = jnp.max(s, axis=1, keepdims=True)
        w = jnp.where(live, jnp.exp(s - top), 0.0)
        tot = jnp.sum(w, axis=1, keepdims=True)
        vs = dot(w.astype(BF16), v_v[b], NT)
        msg = jnp.where(ghalf32, vs, jnp.where(lane32 == mlane32, top, tot))
        stage4[b] = msg
    buf4[:, pl.ds(tp, 1)] = stage4[:, pl.ds(tp, 1)]
    send(3, "tp", (), lambda p: stage4.at[:, pl.ds(p, 1)], buf4.at[:, pl.ds(tp, 1)])

    def merge(y2):
        n = y2.shape[0]
        at_m = iota((n, 128), 1) == mlane
        m = jnp.sum(jnp.where(at_m, y2, 0.0), axis=1, keepdims=True)
        top2 = jnp.max(m, axis=0, keepdims=True)
        zsum = jnp.sum(jnp.exp(m - top2) * y2, axis=0, keepdims=True)
        return jnp.where(lane1 == mlane, top2, zsum)

    c_wo.wait()
    sent(2, buf3.at[:, pl.ds(0, NTP - 1)])
    arrived(3, buf4.at[:, pl.ds(0, NTP - 1)])
    for b in range(3):
        buf5[b, pl.ds(kv, 1)] = merge(buf4[b])
    send(4, "kv", kv_peers, lambda p: buf5.at[:, pl.ds(kv, 1)], buf5.at[:, pl.ds(kv, 1)])
    sent(3, buf4.at[:, pl.ds(0, NTP - 1)])
    arrived(4, buf5.at[:, pl.ds(0, NKV - 1)])
    zrow = jnp.concatenate(
        [merge(buf5[b]) for b in range(3)] + [jnp.ones((5, 128), F32)], axis=0)
    m8 = jnp.sum(jnp.where(lane8 == mlane, zrow, 0.0), axis=1, keepdims=True) + log_gate
    l8 = jnp.sum(jnp.where(lane8 == mlane + 1, zrow, 0.0), axis=1, keepdims=True)
    top8 = jnp.maximum(m8, own)
    a8 = jnp.exp(m8 - top8)
    o8 = jnp.exp(own - top8)
    heads = (zrow * a8 + o8 * v8) / (l8 * a8 + o8)
    heads = jnp.where(ghalf8 & (row8 < 3), heads, 0.0)
    mean = jnp.sum(heads * heads, axis=1, keepdims=True) * (1.0 / HD)
    normed = heads * lax.rsqrt(mean + EPS) * og
    n_lo = normed.astype(BF16)
    n_hi = pltpu.roll(normed, 4, 0).astype(BF16)
    attn = dot(n_lo, wo[:, :128], NN) + dot(n_hi, wo[:, 128:], NN)
    buf6[pl.ds(tp, 1)] = attn.astype(BF16).reshape(1, 8, 128)
    send(5, "tp", (), lambda p: buf6.at[tp], buf6.at[tp])
    c_wg.wait()
    c_wu.wait()
    c_wd.wait()
    sent(4, buf5.at[:, pl.ds(0, NKV - 1)])
    arrived(5, buf6.at[pl.ds(0, NTP - 1)])
    attn8 = jnp.sum(buf6[...].astype(F32), axis=0)
    res8 = (tok8 + attn8).astype(BF16).astype(F32)
    sc8 = (res8 * gain8).astype(BF16).astype(F32)
    sw8 = pltpu.roll(sc8, 4, 0)
    low = row8 < 4
    lhs_g = jnp.concatenate([jnp.where(low, sc8, 0.0), jnp.where(low, sw8, 0.0)], axis=1).astype(BF16)
    lhs_u = jnp.concatenate([jnp.where(low, 0.0, sw8), jnp.where(low, 0.0, sc8)], axis=1).astype(BF16)
    gu = dot(lhs_g, wg[...], NT) + dot(lhs_u, wu[...], NT)
    sq2 = jnp.sum(res8 * res8, axis=1, keepdims=True) + jnp.zeros((8, 128), F32)
    sq2 = sq2 + pltpu.roll(sq2, 4, 0)
    sq2_hi = sq2.astype(BF16).astype(F32)
    lane_t = lane8 + 256
    tail = jnp.where(lane_t == FF_DEV, sq2_hi, jnp.where(lane_t == FF_DEV + 1, sq2 - sq2_hi, gu[:, 256:]))
    gu = jnp.concatenate([gu[:, :256], tail], axis=1)
    buf7[pl.ds(kv, 1)] = gu.astype(BF16).reshape(1, 8, FF_PAD)
    send(6, "kv", kv_peers, lambda p: buf7.at[kv], buf7.at[kv])

    i64 = iota((64, 256), 0)
    n64 = iota((64, 256), 1)
    res_rows = jnp.concatenate([res8, pltpu.roll(res8, 4, 0)], axis=1)
    rep = jnp.broadcast_to(res_rows.reshape(8, 1, 256), (8, 8, 256)).reshape(64, 256)
    diag = (i64 % 8) == (n64 % 8)
    mine = jnp.where(iota((8, 256), 1) // 8 == tp, 1.0, 0.0).astype(BF16)
    res_mine = dot(mine, jnp.where(diag, rep, 0.0).astype(BF16), NT)[0:1]
    fold = jnp.where(iota((32, 256), 1) // 8 == iota((32, 256), 0), 1.0, 0.0).astype(BF16)

    sent(5, buf6.at[pl.ds(0, NTP - 1)])
    arrived(6, buf7.at[pl.ds(0, NKV - 1)])
    gs = jnp.sum(buf7[...].astype(F32), axis=0)
    tail = gs[:, 256:]
    sq2 = jnp.sum(
        jnp.where((lane_t == FF_DEV) | (lane_t == FF_DEV + 1), tail, 0.0), axis=1, keepdims=True)
    rms2 = lax.rsqrt(sq2 * (1.0 / D) + EPS)
    gs = gs * jnp.concatenate([rms2[0:4], rms2[0:4]], axis=0)
    up = pltpu.roll(gs, 4, 0)
    hid = gs / (1.0 + jnp.exp(-gs)) * up
    hid = jnp.where((iota((8, FF_PAD), 1) < FF_DEV) & (iota((8, FF_PAD), 0) < 3), hid, 0.0)
    hid = jnp.broadcast_to(hid.reshape(8, 1, FF_PAD), (8, 8, FF_PAD)).reshape(64, FF_PAD)
    down = dot(hid.astype(BF16), wd[...], NN)
    down = jnp.where(diag, down, 0.0)
    d_hi = down.astype(BF16)
    d_lo = (down - d_hi.astype(F32)).astype(BF16)
    parts = dot(fold, d_hi, NT) + dot(fold, d_lo, NT)
    parts = jnp.concatenate([parts, jnp.zeros((32, 64), F32)], axis=1)
    stage8[...] = parts.reshape(32, 1, 128)
    buf8[pl.ds(tp, 1)] = stage8[pl.ds(tp, 1)]
    send(7, "tp", (), lambda p: stage8.at[p], buf8.at[tp])
    sent(6, buf7.at[pl.ds(0, NKV - 1)])
    arrived(7, buf8.at[pl.ds(0, NTP - 1)])
    share = jnp.sum(buf8[...], axis=0)[:, :64] + res_mine
    out[...] = jnp.concatenate([share[:, 0:8], share[:, 8:16], share[:, 16:24]], axis=0).astype(BF16)
    sent(7, buf8.at[pl.ds(0, NTP - 1)])


def body(
    tokens, lengths, attn_gain, w_query, w_key, w_value, w_forget, forget_bias,
    cache_keys, cache_values, cache_decay, out_gain, w_out, mlp_gain, w_gate, w_up, w_down,
):
    hbm = pl.BlockSpec(memory_space=pl.ANY)
    v = pltpu.VMEM
    return pl.pallas_call(
        kernel,
        out_shape=pltpu.VMEM((3, 8), BF16),
        in_specs=[hbm] * 17,
        out_specs=pl.BlockSpec(memory_space=pltpu.VMEM),
        scratch_shapes=[
            pltpu.SMEM((3,), jnp.int32), v((3, 8), BF16), v((1, 8), F32), v((1, 8), F32), v((1, 32), F32), v((16, 128), F32),
            v((128, 256), BF16), v((256, 128), BF16), v((256, 128), BF16), v((256, 128), BF16),
            v((3, 128, SPAN), BF16), v((3, 128, SPAN), BF16), v((3, 32, SPAN), F32),
            v((128, 256), BF16),
            v((FF_PAD, 256), BF16), v((FF_PAD, 256), BF16), v((FF_PAD, 256), BF16),
            v((NTP, 1, 128), F32), v((NKV, 8, 128), F32), v((3, NTP, 128), F32),
            v((3, NTP, 128), F32), v((3, NTP, 128), F32), v((3, NKV, 128), F32),
            v((NTP, 8, 128), BF16), v((NKV, 8, FF_PAD), BF16),
            v((NTP, 1, 128), F32), v((NTP, 1, 128), F32),
            pltpu.SemaphoreType.DMA((17,)),
            pltpu.SemaphoreType.DMA((8,)),
            pltpu.SemaphoreType.DMA((8,)),
            pltpu.SemaphoreType.REGULAR,
        ],
        compiler_params=pltpu.CompilerParams(
            collective_id=0, has_side_effects=True, vmem_limit_bytes=60 * 1024 * 1024),
    )(
        lengths, tokens, attn_gain.reshape(1, 8), mlp_gain.reshape(1, 8),
        forget_bias.reshape(1, 32), out_gain.reshape(16, 128),
        w_query.T, w_key, w_value, w_forget.T, cache_keys, cache_values, cache_decay, w_out,
        w_gate.T, w_up.T, w_down,
    )


def solution(mesh):
    kvtp = ("kv", "tp")
    placed = (
        P(None, kvtp), P(), P(kvtp), P("kv", "tp"), P("kv", None), P("kv", None), P(), P(),
        P(None, None, kvtp), P(None, None, kvtp), P(None, None, kvtp), P(), P("tp", "kv"),
        P(kvtp), P("kv", "tp"), P("kv", "tp"), P("tp", "kv"),
    )
    return jax.shard_map(
        body, mesh=mesh, in_specs=placed, out_specs=P(None, kvtp), check_vma=False)
```

```python
import jax
import jax.numpy as jnp
from jax import lax
from jax.experimental import pallas as pl
from jax.experimental.pallas import tpu as pltpu
from jax.sharding import PartitionSpec as P

MESH = pl.DeviceIdType.MESH
D = 4096
HD = 64
NTP = 32
NKV = 16
FF_DEV = 352
FF_PAD = 384
SPAN = 256
EPS = 1e-06
MASKED = -1e30
F32 = jnp.float32
BF16 = jnp.bfloat16

NT = (((1,), (1,)), ((), ()))
NN = (((1,), (0,)), ((), ()))

def dot(a, b, dims, **kw):
    return lax.dot_general(a, b, dims, preferred_element_type=F32, **kw)


def iota(shape, dim):
    return lax.broadcasted_iota(jnp.int32, shape, dim)


def kernel(
    lengths_h, tokens, attn_gain, mlp_gain, forget_bias, out_gain,
    w_query, w_key, w_value, w_forget, keys, values, decay, w_out,
    w_gate, w_up, w_down,
    out,
    lengths, tok_v, ag_v, mg_v, fb_v, og_v, wqf, wk, wv, wkv, k_v, v_v, d_v, wo,
    wg, wu, wd,
    buf1, buf2, buf3, stage4, buf4, buf5, buf6, buf7, stage8, buf8,
    lsem, ssem, rsem, pair_ready,
):
    kv = lax.axis_index("kv")
    tp = lax.axis_index("tp")
    g = tp // 16
    z = tp // 2
    core = tp % 2
    y = kv // 4
    x = kv % 4

    kv_peers = []
    for dist in (4, 3, 2, 1):
        for dy in (2, 1, 3, 0):
            for dx in (2, 1, 3, 0):
                if min(dy, 4 - dy) + min(dx, 4 - dx) == dist:
                    kv_peers.append(lax.rem(y + dy, 4) * 4 + lax.rem(x + dx, 4))

    barrier = pltpu.get_barrier_semaphore()

    def far_peer(i):
        s = i // 2
        d = 8 - (s + 1) // 2
        return lax.rem(z + d + (16 - 2 * d) * (1 - s % 2), 16) * 2 + lax.rem(core + i, 2)

    def greet(s, carry):
        pl.semaphore_signal(barrier, inc=1, device_id={"tp": far_peer(2 * s)}, device_id_type=MESH)
        return carry
    lax.fori_loop(0, 15, greet, 0)
    partner = z * 2 + (1 - core)
    pl.semaphore_signal(barrier, inc=1, device_id={"tp": partner}, device_id_type=MESH)
    for p in kv_peers:
        pl.semaphore_signal(barrier, inc=1, device_id={"kv": p}, device_id_type=MESH)

    def load(i, src, dst):
        c = pltpu.make_async_copy(src, dst, lsem.at[i])
        c.start()
        return c

    half = pl.multiple_of(g * HD, HD)
    other = pl.multiple_of((1 - g) * HD, HD)
    c_tok = load(0, tokens, tok_v)
    c_ag = load(1, attn_gain, ag_v)
    c_mg = load(2, mlp_gain, mg_v)
    c_wq = load(3, w_query, wqf.at[pl.ds(half, HD)])
    cols = pl.ds(pl.multiple_of(kv * 256, 256), 256)
    c_wf = load(4, w_forget.at[:, cols], wqf.at[pl.ds(other, 32)])
    c_wk = load(5, w_key, wk)
    c_wv = load(6, w_value, wv)
    c_k = load(7, keys, k_v)
    c_d = load(8, decay, d_v)
    c_v = load(9, values, v_v)
    c_fb = load(10, forget_bias, fb_v)
    c_og = load(11, out_gain, og_v)
    c_wo = load(12, w_out, wo.at[pl.ds(half, HD)])
    c_wg = load(13, w_gate, wg.at[pl.ds(0, FF_DEV)])
    c_wu = load(14, w_up, wu.at[pl.ds(0, FF_DEV)])
    c_wd = load(15, w_down, wd.at[pl.ds(0, FF_DEV)])
    c_len = load(16, lengths_h, lengths)

    def send(n, axis, peers, src, dst):
        def one(p):
            pltpu.make_async_remote_copy(
                src_ref=src(p), dst_ref=dst, send_sem=ssem.at[n], recv_sem=rsem.at[n],
                device_id={axis: p}, device_id_type=MESH,
            ).start()
        if axis == "kv":
            for p in peers:
                one(p)
            return

        def step(i, carry):
            one(far_peer(i))
            return carry
        lax.fori_loop(0, 30, step, 0)
        one(partner)

    def arrived(n, ref):
        pltpu.make_async_copy(ref, ref, rsem.at[n]).wait()

    def sent(n, ref):
        pltpu.make_async_copy(ref, ref, ssem.at[n]).wait()

    lane8 = iota((8, 128), 1)
    row8 = iota((8, 128), 0)
    lane1 = iota((1, 128), 1)
    ghalf8 = (lane8 // HD) == g
    mlane = (1 - g) * HD

    c_tok.wait()
    c_ag.wait()
    c_mg.wait()
    tok = tok_v[...].astype(F32)
    scaled = (tok * ag_v[...]).astype(BF16).astype(F32)
    row = jnp.concatenate(
        [scaled[0:1], scaled[1:2], scaled[2:3], tok[0:1], tok[1:2], tok[2:3], mg_v[...],
         jnp.zeros((1, 72), F32)], axis=1)
    buf1[pl.ds(tp, 1)] = row.reshape(1, 1, 128)

    wqf[pl.ds(other + 32, 32)] = jnp.zeros((32, 256), BF16)
    wo[pl.ds(other, HD)] = jnp.zeros((HD, 256), BF16)
    for w in (wg, wu, wd):
        w[FF_DEV:] = jnp.zeros((FF_PAD - FF_DEV, 256), BF16)
    c_wk.wait()
    c_wv.wait()
    wkv[...] = jnp.where(
        (iota((256, 128), 1) // HD) == g,
        wk[...].astype(F32), pltpu.roll(wv[...].astype(F32), HD, 1)).astype(BF16)
    c_wq.wait()
    c_wf.wait()

    pl.semaphore_wait(barrier, 16 + len(kv_peers))
    pl.semaphore_signal(pair_ready, inc=1, device_id={"tp": partner}, device_id_type=MESH)

    pl.semaphore_wait(pair_ready, 1)
    send(0, "tp", (), lambda p: buf1.at[tp], buf1.at[tp])
    r24 = iota((24, 128), 0)
    b24 = r24 % 4
    want24 = jnp.where(
        r24 < 16,
        jnp.where((r24 < 4) | ((r24 >= 12) & (r24 < 16)), b24, -1),
        b24 + 3)
    l24 = iota((24, 128), 1)
    sel = jnp.where((b24 < 3) & (l24 // 8 == want24), 1.0, 0.0).astype(BF16)
    spread = (iota((256, 128), 0) % 8) == (iota((256, 128), 1) % 8)
    arrived(0, buf1.at[pl.ds(0, NTP - 1)])
    block = jnp.broadcast_to(buf1[...], (NTP, 8, 128)).reshape(256, 128)
    block = jnp.where(spread, block, 0.0)
    rows = dot(sel, block.astype(BF16), NT)
    tok_rows = rows[16:24]
    part = dot(rows[0:8].astype(BF16), wqf[...], NT) + dot(rows[8:16].astype(BF16), wkv[...], NN)
    squares = jnp.sum(tok_rows * tok_rows, axis=1, keepdims=True)
    part = jnp.where((lane8 == mlane + 32) & (row8 < 4), squares, part)
    buf2[pl.ds(kv, 1)] = part.reshape(1, 8, 128)
    send(1, "kv", kv_peers, lambda p: buf2.at[kv], buf2.at[kv])

    tok8 = jnp.where(row8 < 4, tok_rows[:, :128], tok_rows[:, 128:])
    gsel = jnp.where(lane8 // 8 == 6, 1.0, 0.0)
    gain_rows = dot(gsel, block, NT, precision=lax.Precision.HIGHEST)
    gain8 = jnp.where(row8 < 4, gain_rows[:, :128], gain_rows[:, 128:])
    c_fb.wait()
    c_og.wait()
    bias_row = jnp.concatenate([fb_v[...], jnp.zeros((1, 96), F32)], axis=1)
    bias = jnp.sum(jnp.where(lane1 == tp, bias_row, 0.0), axis=1, keepdims=True)
    og = og_v[pl.ds(z, 1)]
    og = jnp.where(core == g, og, pltpu.roll(og, HD, 1))

    sent(0, buf1.at[pl.ds(0, NTP - 1)])
    arrived(1, buf2.at[pl.ds(0, NKV - 1)])
    total8 = jnp.sum(buf2[...], axis=0)
    sq = jnp.sum(jnp.where(lane8 == mlane + 32, total8, 0.0), axis=1, keepdims=True)
    rms1 = lax.rsqrt(sq * (1.0 / D) + EPS)
    q8 = jnp.where(ghalf8 & (row8 < 3), (total8 * rms1).astype(BF16).astype(F32), 0.0)
    for b in range(3):
        buf3[b, pl.ds(tp, 1)] = q8[b:b + 1]
    send(2, "tp", (), lambda p: buf3.at[:, pl.ds(tp, 1)], buf3.at[:, pl.ds(tp, 1)])

    kv8 = (pltpu.roll(total8, 4, 0) * rms1).astype(BF16).astype(F32)
    own = jnp.sum(q8 * kv8, axis=1, keepdims=True) * (HD ** -0.5)
    v8 = pltpu.roll(kv8, HD, 1)
    fj = jnp.sum(jnp.where(lane8 == mlane + tp, total8, 0.0), axis=1, keepdims=True) * rms1 + bias
    log_gate = jnp.minimum(fj, 0.0) - jnp.log1p(jnp.exp(-jnp.abs(fj)))
    c_k.wait()
    c_d.wait()
    c_v.wait()
    c_len.wait()
    positions = (kv * NTP + tp) * SPAN + iota((32, SPAN), 1)
    lane32 = iota((32, 128), 1)
    ghalf32 = (lane32 // HD) == (iota((32, 128), 0) // 16)
    mlane32 = (1 - iota((32, 128), 0) // 16) * HD

    sent(1, buf2.at[pl.ds(0, NKV - 1)])
    arrived(2, buf3.at[:, pl.ds(0, NTP - 1)])
    for b in range(3):
        qb = buf3[b].astype(BF16)
        s = dot(qb, k_v[b], NN) * (HD ** -0.5) + d_v[b]
        live = positions < lengths[b]
        s = jnp.where(live, s, MASKED)
        top = jnp.max(s, axis=1, keepdims=True)
        w = jnp.where(live, jnp.exp(s - top), 0.0)
        tot = jnp.sum(w, axis=1, keepdims=True)
        vs = dot(w.astype(BF16), v_v[b], NT)
        msg = jnp.where(ghalf32, vs, jnp.where(lane32 == mlane32, top, tot))
        stage4[b] = msg
    buf4[:, pl.ds(tp, 1)] = stage4[:, pl.ds(tp, 1)]
    send(3, "tp", (), lambda p: stage4.at[:, pl.ds(p, 1)], buf4.at[:, pl.ds(tp, 1)])

    def merge(y2):
        n = y2.shape[0]
        at_m = iota((n, 128), 1) == mlane
        m = jnp.sum(jnp.where(at_m, y2, 0.0), axis=1, keepdims=True)
        top2 = jnp.max(m, axis=0, keepdims=True)
        zsum = jnp.sum(jnp.exp(m - top2) * y2, axis=0, keepdims=True)
        return jnp.where(lane1 == mlane, top2, zsum)

    c_wo.wait()
    sent(2, buf3.at[:, pl.ds(0, NTP - 1)])
    arrived(3, buf4.at[:, pl.ds(0, NTP - 1)])
    for b in range(3):
        buf5[b, pl.ds(kv, 1)] = merge(buf4[b])
    send(4, "kv", kv_peers, lambda p: buf5.at[:, pl.ds(kv, 1)], buf5.at[:, pl.ds(kv, 1)])
    sent(3, buf4.at[:, pl.ds(0, NTP - 1)])
    arrived(4, buf5.at[:, pl.ds(0, NKV - 1)])
    zrow = jnp.concatenate(
        [merge(buf5[b]) for b in range(3)] + [jnp.ones((5, 128), F32)], axis=0)
    m8 = jnp.sum(jnp.where(lane8 == mlane, zrow, 0.0), axis=1, keepdims=True) + log_gate
    l8 = jnp.sum(jnp.where(lane8 == mlane + 1, zrow, 0.0), axis=1, keepdims=True)
    top8 = jnp.maximum(m8, own)
    a8 = jnp.exp(m8 - top8)
    o8 = jnp.exp(own - top8)
    heads = (zrow * a8 + o8 * v8) / (l8 * a8 + o8)
    heads = jnp.where(ghalf8 & (row8 < 3), heads, 0.0)
    mean = jnp.sum(heads * heads, axis=1, keepdims=True) * (1.0 / HD)
    normed = heads * lax.rsqrt(mean + EPS) * og
    n_lo = normed.astype(BF16)
    n_hi = pltpu.roll(normed, 4, 0).astype(BF16)
    attn = dot(n_lo, wo[:, :128], NN) + dot(n_hi, wo[:, 128:], NN)
    buf6[pl.ds(tp, 1)] = attn.astype(BF16).reshape(1, 8, 128)
    send(5, "tp", (), lambda p: buf6.at[tp], buf6.at[tp])
    c_wg.wait()
    c_wu.wait()
    c_wd.wait()
    sent(4, buf5.at[:, pl.ds(0, NKV - 1)])
    arrived(5, buf6.at[pl.ds(0, NTP - 1)])
    attn8 = jnp.sum(buf6[...].astype(F32), axis=0)
    res8 = (tok8 + attn8).astype(BF16).astype(F32)
    sc8 = (res8 * gain8).astype(BF16).astype(F32)
    sw8 = pltpu.roll(sc8, 4, 0)
    low = row8 < 4
    lhs_g = jnp.concatenate([jnp.where(low, sc8, 0.0), jnp.where(low, sw8, 0.0)], axis=1).astype(BF16)
    lhs_u = jnp.concatenate([jnp.where(low, 0.0, sw8), jnp.where(low, 0.0, sc8)], axis=1).astype(BF16)
    gu = dot(lhs_g, wg[...], NT) + dot(lhs_u, wu[...], NT)
    sq2 = jnp.sum(res8 * res8, axis=1, keepdims=True) + jnp.zeros((8, 128), F32)
    sq2 = sq2 + pltpu.roll(sq2, 4, 0)
    sq2_hi = sq2.astype(BF16).astype(F32)
    lane_t = lane8 + 256
    tail = jnp.where(lane_t == FF_DEV, sq2_hi, jnp.where(lane_t == FF_DEV + 1, sq2 - sq2_hi, gu[:, 256:]))
    gu = jnp.concatenate([gu[:, :256], tail], axis=1)
    buf7[pl.ds(kv, 1)] = gu.astype(BF16).reshape(1, 8, FF_PAD)
    send(6, "kv", kv_peers, lambda p: buf7.at[kv], buf7.at[kv])

    i64 = iota((64, 256), 0)
    n64 = iota((64, 256), 1)
    res_rows = jnp.concatenate([res8, pltpu.roll(res8, 4, 0)], axis=1)
    rep = jnp.broadcast_to(res_rows.reshape(8, 1, 256), (8, 8, 256)).reshape(64, 256)
    diag = (i64 % 8) == (n64 % 8)
    mine = jnp.where(iota((8, 256), 1) // 8 == tp, 1.0, 0.0).astype(BF16)
    res_mine = dot(mine, jnp.where(diag, rep, 0.0).astype(BF16), NT)[0:1]
    fold = jnp.where(iota((32, 256), 1) // 8 == iota((32, 256), 0), 1.0, 0.0).astype(BF16)

    sent(5, buf6.at[pl.ds(0, NTP - 1)])
    arrived(6, buf7.at[pl.ds(0, NKV - 1)])
    gs = jnp.sum(buf7[...].astype(F32), axis=0)
    tail = gs[:, 256:]
    sq2 = jnp.sum(
        jnp.where((lane_t == FF_DEV) | (lane_t == FF_DEV + 1), tail, 0.0), axis=1, keepdims=True)
    rms2 = lax.rsqrt(sq2 * (1.0 / D) + EPS)
    gs = gs * jnp.concatenate([rms2[0:4], rms2[0:4]], axis=0)
    up = pltpu.roll(gs, 4, 0)
    hid = gs / (1.0 + jnp.exp(-gs)) * up
    hid = jnp.where((iota((8, FF_PAD), 1) < FF_DEV) & (iota((8, FF_PAD), 0) < 3), hid, 0.0)
    hid = jnp.broadcast_to(hid.reshape(8, 1, FF_PAD), (8, 8, FF_PAD)).reshape(64, FF_PAD)
    down = dot(hid.astype(BF16), wd[...], NN)
    down = jnp.where(diag, down, 0.0)
    d_hi = down.astype(BF16)
    d_lo = (down - d_hi.astype(F32)).astype(BF16)
    parts = dot(fold, d_hi, NT) + dot(fold, d_lo, NT)
    parts = jnp.concatenate([parts, jnp.zeros((32, 64), F32)], axis=1)
    stage8[...] = parts.reshape(32, 1, 128)
    buf8[pl.ds(tp, 1)] = stage8[pl.ds(tp, 1)]
    send(7, "tp", (), lambda p: stage8.at[p], buf8.at[tp])
    sent(6, buf7.at[pl.ds(0, NKV - 1)])
    arrived(7, buf8.at[pl.ds(0, NTP - 1)])
    share = jnp.sum(buf8[...], axis=0)[:, :64] + res_mine
    out[...] = jnp.concatenate([share[:, 0:8], share[:, 8:16], share[:, 16:24]], axis=0).astype(BF16)
    sent(7, buf8.at[pl.ds(0, NTP - 1)])


def body(
    tokens, lengths, attn_gain, w_query, w_key, w_value, w_forget, forget_bias,
    cache_keys, cache_values, cache_decay, out_gain, w_out, mlp_gain, w_gate, w_up, w_down,
):
    hbm = pl.BlockSpec(memory_space=pl.ANY)
    v = pltpu.VMEM
    return pl.pallas_call(
        kernel,
        out_shape=pltpu.VMEM((3, 8), BF16),
        in_specs=[hbm] * 17,
        out_specs=pl.BlockSpec(memory_space=pltpu.VMEM),
        scratch_shapes=[
            pltpu.SMEM((3,), jnp.int32), v((3, 8), BF16), v((1, 8), F32), v((1, 8), F32), v((1, 32), F32), v((16, 128), F32),
            v((128, 256), BF16), v((256, 128), BF16), v((256, 128), BF16), v((256, 128), BF16),
            v((3, 128, SPAN), BF16), v((3, 128, SPAN), BF16), v((3, 32, SPAN), F32),
            v((128, 256), BF16),
            v((FF_PAD, 256), BF16), v((FF_PAD, 256), BF16), v((FF_PAD, 256), BF16),
            v((NTP, 1, 128), F32), v((NKV, 8, 128), F32), v((3, NTP, 128), F32),
            v((3, NTP, 128), F32), v((3, NTP, 128), F32), v((3, NKV, 128), F32),
            v((NTP, 8, 128), BF16), v((NKV, 8, FF_PAD), BF16),
            v((NTP, 1, 128), F32), v((NTP, 1, 128), F32),
            pltpu.SemaphoreType.DMA((17,)),
            pltpu.SemaphoreType.DMA((8,)),
            pltpu.SemaphoreType.DMA((8,)),
            pltpu.SemaphoreType.REGULAR,
        ],
        compiler_params=pltpu.CompilerParams(
            collective_id=0, has_side_effects=True, vmem_limit_bytes=60 * 1024 * 1024),
    )(
        lengths, tokens, attn_gain.reshape(1, 8), mlp_gain.reshape(1, 8),
        forget_bias.reshape(1, 32), out_gain.reshape(16, 128),
        w_query.T, w_key, w_value, w_forget.T, cache_keys, cache_values, cache_decay, w_out,
        w_gate.T, w_up.T, w_down,
    )


def solution(mesh):
    kvtp = ("kv", "tp")
    placed = (
        P(None, kvtp), P(), P(kvtp), P("kv", "tp"), P("kv", None), P("kv", None), P(), P(),
        P(None, None, kvtp), P(None, None, kvtp), P(None, None, kvtp), P(), P("tp", "kv"),
        P(kvtp), P("kv", "tp"), P("kv", "tp"), P("tp", "kv"),
    )
    return jax.shard_map(
        body, mesh=mesh, in_specs=placed, out_specs=P(None, kvtp), check_vma=False)
```

```python
import jax
import jax.numpy as jnp
from jax import lax
from jax.experimental import pallas as pl
from jax.experimental.pallas import tpu as pltpu
from jax.sharding import PartitionSpec as P

MESH = pl.DeviceIdType.MESH
D = 4096
HD = 64
NTP = 32
NKV = 16
FF_DEV = 352
FF_PAD = 384
SPAN = 256
EPS = 1e-06
MASKED = -1e30
F32 = jnp.float32
BF16 = jnp.bfloat16

NT = (((1,), (1,)), ((), ()))
NN = (((1,), (0,)), ((), ()))

def dot(a, b, dims, **kw):
    return lax.dot_general(a, b, dims, preferred_element_type=F32, **kw)


def iota(shape, dim):
    return lax.broadcasted_iota(jnp.int32, shape, dim)


def kernel(
    lengths_h, tokens, attn_gain, mlp_gain, forget_bias, out_gain,
    w_query, w_key, w_value, w_forget, keys, values, decay, w_out,
    w_gate, w_up, w_down,
    out,
    lengths, tok_v, ag_v, mg_v, fb_v, og_v, wqf, wk, wv, wkv, k_v, v_v, d_v, wo,
    wg, wu, wd,
    buf1, buf2, buf3, stage4, buf4, buf5, buf6, buf7, stage8, buf8,
    lsem, ssem, rsem, pair_ready,
):
    kv = lax.axis_index("kv")
    tp = lax.axis_index("tp")
    g = tp // 16
    z = tp // 2
    core = tp % 2
    y = kv // 4
    x = kv % 4

    kv_peers = []
    for dist in (4, 3, 2, 1):
        for dy in (2, 1, 3, 0):
            for dx in (2, 1, 3, 0):
                if min(dy, 4 - dy) + min(dx, 4 - dx) == dist:
                    kv_peers.append(lax.rem(y + dy, 4) * 4 + lax.rem(x + dx, 4))

    barrier = pltpu.get_barrier_semaphore()

    def far_peer(i):
        s = i // 2
        d = 8 - (s + 1) // 2
        return lax.rem(z + d + (16 - 2 * d) * (1 - s % 2), 16) * 2 + lax.rem(core + i, 2)

    def greet(s, carry):
        pl.semaphore_signal(barrier, inc=1, device_id={"tp": far_peer(2 * s)}, device_id_type=MESH)
        return carry
    lax.fori_loop(0, 15, greet, 0)
    partner = z * 2 + (1 - core)
    pl.semaphore_signal(barrier, inc=1, device_id={"tp": partner}, device_id_type=MESH)
    for p in kv_peers:
        pl.semaphore_signal(barrier, inc=1, device_id={"kv": p}, device_id_type=MESH)

    def load(i, src, dst):
        c = pltpu.make_async_copy(src, dst, lsem.at[i])
        c.start()
        return c

    half = pl.multiple_of(g * HD, HD)
    other = pl.multiple_of((1 - g) * HD, HD)
    c_tok = load(0, tokens, tok_v)
    c_ag = load(1, attn_gain, ag_v)
    c_mg = load(2, mlp_gain, mg_v)
    c_wq = load(3, w_query, wqf.at[pl.ds(half, HD)])
    cols = pl.ds(pl.multiple_of(kv * 256, 256), 256)
    c_wf = load(4, w_forget.at[:, cols], wqf.at[pl.ds(other, 32)])
    c_wk = load(5, w_key, wk)
    c_wv = load(6, w_value, wv)
    c_k = load(7, keys, k_v)
    c_d = load(8, decay, d_v)
    c_v = load(9, values, v_v)
    c_fb = load(10, forget_bias, fb_v)
    c_og = load(11, out_gain, og_v)
    c_wo = load(12, w_out, wo.at[pl.ds(half, HD)])
    c_wg = load(13, w_gate, wg.at[pl.ds(0, FF_DEV)])
    c_wu = load(14, w_up, wu.at[pl.ds(0, FF_DEV)])
    c_wd = load(15, w_down, wd.at[pl.ds(0, FF_DEV)])
    c_len = load(16, lengths_h, lengths)

    def send(n, axis, peers, src, dst):
        def one(p):
            pltpu.make_async_remote_copy(
                src_ref=src(p), dst_ref=dst, send_sem=ssem.at[n], recv_sem=rsem.at[n],
                device_id={axis: p}, device_id_type=MESH,
            ).start()
        if axis == "kv":
            for p in peers:
                one(p)
            return

        def step(i, carry):
            one(far_peer(i))
            return carry
        lax.fori_loop(0, 30, step, 0)
        one(partner)

    def arrived(n, ref):
        pltpu.make_async_copy(ref, ref, rsem.at[n]).wait()

    def sent(n, ref):
        pltpu.make_async_copy(ref, ref, ssem.at[n]).wait()

    lane8 = iota((8, 128), 1)
    row8 = iota((8, 128), 0)
    lane1 = iota((1, 128), 1)
    ghalf8 = (lane8 // HD) == g
    mlane = (1 - g) * HD

    c_tok.wait()
    c_ag.wait()
    c_mg.wait()
    tok = tok_v[...].astype(F32)
    scaled = (tok * ag_v[...]).astype(BF16).astype(F32)
    row = jnp.concatenate(
        [scaled[0:1], scaled[1:2], scaled[2:3], tok[0:1], tok[1:2], tok[2:3], mg_v[...],
         jnp.zeros((1, 72), F32)], axis=1)
    buf1[pl.ds(tp, 1)] = row.reshape(1, 1, 128)

    wqf[pl.ds(other + 32, 32)] = jnp.zeros((32, 256), BF16)
    wo[pl.ds(other, HD)] = jnp.zeros((HD, 256), BF16)
    for w in (wg, wu, wd):
        w[FF_DEV:] = jnp.zeros((FF_PAD - FF_DEV, 256), BF16)
    c_wk.wait()
    c_wv.wait()
    wkv[...] = jnp.where(
        (iota((256, 128), 1) // HD) == g,
        wk[...].astype(F32), pltpu.roll(wv[...].astype(F32), HD, 1)).astype(BF16)
    c_wq.wait()
    c_wf.wait()

    pl.semaphore_wait(barrier, 16 + len(kv_peers))
    pl.semaphore_signal(pair_ready, inc=1, device_id={"tp": partner}, device_id_type=MESH)

    pl.semaphore_wait(pair_ready, 1)
    send(0, "tp", (), lambda p: buf1.at[tp], buf1.at[tp])
    r24 = iota((24, 128), 0)
    b24 = r24 % 4
    want24 = jnp.where(
        r24 < 16,
        jnp.where((r24 < 4) | ((r24 >= 12) & (r24 < 16)), b24, -1),
        b24 + 3)
    l24 = iota((24, 128), 1)
    sel = jnp.where((b24 < 3) & (l24 // 8 == want24), 1.0, 0.0).astype(BF16)
    spread = (iota((256, 128), 0) % 8) == (iota((256, 128), 1) % 8)
    arrived(0, buf1.at[pl.ds(0, NTP - 1)])
    block = jnp.broadcast_to(buf1[...], (NTP, 8, 128)).reshape(256, 128)
    block = jnp.where(spread, block, 0.0)
    rows = dot(sel, block.astype(BF16), NT)
    tok_rows = rows[16:24]
    part = dot(rows[0:8].astype(BF16), wqf[...], NT) + dot(rows[8:16].astype(BF16), wkv[...], NN)
    squares = jnp.sum(tok_rows * tok_rows, axis=1, keepdims=True)
    part = jnp.where((lane8 == mlane + 32) & (row8 < 4), squares, part)
    buf2[pl.ds(kv, 1)] = part.reshape(1, 8, 128)
    send(1, "kv", kv_peers, lambda p: buf2.at[kv], buf2.at[kv])

    tok8 = jnp.where(row8 < 4, tok_rows[:, :128], tok_rows[:, 128:])
    gsel = jnp.where(lane8 // 8 == 6, 1.0, 0.0)
    gain_rows = dot(gsel, block, NT, precision=lax.Precision.HIGHEST)
    gain8 = jnp.where(row8 < 4, gain_rows[:, :128], gain_rows[:, 128:])
    c_fb.wait()
    c_og.wait()
    bias_row = jnp.concatenate([fb_v[...], jnp.zeros((1, 96), F32)], axis=1)
    bias = jnp.sum(jnp.where(lane1 == tp, bias_row, 0.0), axis=1, keepdims=True)
    og = og_v[pl.ds(z, 1)]
    og = jnp.where(core == g, og, pltpu.roll(og, HD, 1))

    sent(0, buf1.at[pl.ds(0, NTP - 1)])
    arrived(1, buf2.at[pl.ds(0, NKV - 1)])
    total8 = jnp.sum(buf2[...], axis=0)
    sq = jnp.sum(jnp.where(lane8 == mlane + 32, total8, 0.0), axis=1, keepdims=True)
    rms1 = lax.rsqrt(sq * (1.0 / D) + EPS)
    q8 = jnp.where(ghalf8 & (row8 < 3), (total8 * rms1).astype(BF16).astype(F32), 0.0)
    for b in range(3):
        buf3[b, pl.ds(tp, 1)] = q8[b:b + 1]
    send(2, "tp", (), lambda p: buf3.at[:, pl.ds(tp, 1)], buf3.at[:, pl.ds(tp, 1)])

    kv8 = (pltpu.roll(total8, 4, 0) * rms1).astype(BF16).astype(F32)
    own = jnp.sum(q8 * kv8, axis=1, keepdims=True) * (HD ** -0.5)
    v8 = pltpu.roll(kv8, HD, 1)
    fj = jnp.sum(jnp.where(lane8 == mlane + tp, total8, 0.0), axis=1, keepdims=True) * rms1 + bias
    log_gate = jnp.minimum(fj, 0.0) - jnp.log1p(jnp.exp(-jnp.abs(fj)))
    c_k.wait()
    c_d.wait()
    c_v.wait()
    c_len.wait()
    positions = (kv * NTP + tp) * SPAN + iota((32, SPAN), 1)
    lane32 = iota((32, 128), 1)
    ghalf32 = (lane32 // HD) == (iota((32, 128), 0) // 16)
    mlane32 = (1 - iota((32, 128), 0) // 16) * HD

    sent(1, buf2.at[pl.ds(0, NKV - 1)])
    for b in range(3):
        d_v[b] = jnp.where(positions < lengths[b], d_v[b], MASKED)
    arrived(2, buf3.at[:, pl.ds(0, NTP - 1)])
    for b in range(3):
        qb = buf3[b].astype(BF16)
        s = dot(qb, k_v[b], NN) * (HD ** -0.5) + d_v[b]
        top = jnp.maximum(jnp.max(s, axis=1, keepdims=True), 0.1 * MASKED)
        w = jnp.exp(s - top)
        tot = jnp.sum(w, axis=1, keepdims=True)
        vs = dot(w.astype(BF16), v_v[b], NT)
        msg = jnp.where(ghalf32, vs, jnp.where(lane32 == mlane32, top, tot))
        stage4[b] = msg
    send(3, "tp", (), lambda p: stage4.at[:, pl.ds(p, 1)], buf4.at[:, pl.ds(tp, 1)])
    buf4[:, pl.ds(tp, 1)] = stage4[:, pl.ds(tp, 1)]

    def merge(y2):
        n = y2.shape[0]
        at_m = iota((n, 128), 1) == mlane
        m = jnp.sum(jnp.where(at_m, y2, 0.0), axis=1, keepdims=True)
        top2 = jnp.max(m, axis=0, keepdims=True)
        zsum = jnp.sum(jnp.exp(m - top2) * y2, axis=0, keepdims=True)
        return jnp.where(lane1 == mlane, top2, zsum)

    c_wo.wait()
    sent(2, buf3.at[:, pl.ds(0, NTP - 1)])
    arrived(3, buf4.at[:, pl.ds(0, NTP - 1)])
    for b in range(3):
        buf5[b, pl.ds(kv, 1)] = merge(buf4[b])
    send(4, "kv", kv_peers, lambda p: buf5.at[:, pl.ds(kv, 1)], buf5.at[:, pl.ds(kv, 1)])
    sent(3, buf4.at[:, pl.ds(0, NTP - 1)])
    arrived(4, buf5.at[:, pl.ds(0, NKV - 1)])
    zrow = jnp.concatenate(
        [merge(buf5[b]) for b in range(3)] + [jnp.ones((5, 128), F32)], axis=0)
    m8 = jnp.sum(jnp.where(lane8 == mlane, zrow, 0.0), axis=1, keepdims=True) + log_gate
    l8 = jnp.sum(jnp.where(lane8 == mlane + 1, zrow, 0.0), axis=1, keepdims=True)
    top8 = jnp.maximum(m8, own)
    a8 = jnp.exp(m8 - top8)
    o8 = jnp.exp(own - top8)
    heads = (zrow * a8 + o8 * v8) / (l8 * a8 + o8)
    heads = jnp.where(ghalf8 & (row8 < 3), heads, 0.0)
    mean = jnp.sum(heads * heads, axis=1, keepdims=True) * (1.0 / HD)
    normed = heads * lax.rsqrt(mean + EPS) * og
    n_lo = normed.astype(BF16)
    n_hi = pltpu.roll(normed, 4, 0).astype(BF16)
    attn = dot(n_lo, wo[:, :128], NN) + dot(n_hi, wo[:, 128:], NN)
    buf6[pl.ds(tp, 1)] = attn.astype(BF16).reshape(1, 8, 128)
    send(5, "tp", (), lambda p: buf6.at[tp], buf6.at[tp])
    c_wg.wait()
    c_wu.wait()
    c_wd.wait()
    sent(4, buf5.at[:, pl.ds(0, NKV - 1)])
    arrived(5, buf6.at[pl.ds(0, NTP - 1)])
    attn8 = jnp.sum(buf6[...].astype(F32), axis=0)
    res8 = (tok8 + attn8).astype(BF16).astype(F32)
    sc8 = (res8 * gain8).astype(BF16).astype(F32)
    sw8 = pltpu.roll(sc8, 4, 0)
    low = row8 < 4
    lhs_g = jnp.concatenate([jnp.where(low, sc8, 0.0), jnp.where(low, sw8, 0.0)], axis=1).astype(BF16)
    lhs_u = jnp.concatenate([jnp.where(low, 0.0, sw8), jnp.where(low, 0.0, sc8)], axis=1).astype(BF16)
    gu = dot(lhs_g, wg[...], NT) + dot(lhs_u, wu[...], NT)
    sq2 = jnp.sum(res8 * res8, axis=1, keepdims=True) + jnp.zeros((8, 128), F32)
    sq2 = sq2 + pltpu.roll(sq2, 4, 0)
    sq2_hi = sq2.astype(BF16).astype(F32)
    lane_t = lane8 + 256
    tail = jnp.where(lane_t == FF_DEV, sq2_hi, jnp.where(lane_t == FF_DEV + 1, sq2 - sq2_hi, gu[:, 256:]))
    gu = jnp.concatenate([gu[:, :256], tail], axis=1)
    buf7[pl.ds(kv, 1)] = gu.astype(BF16).reshape(1, 8, FF_PAD)
    send(6, "kv", kv_peers, lambda p: buf7.at[kv], buf7.at[kv])

    i64 = iota((64, 256), 0)
    n64 = iota((64, 256), 1)
    res_rows = jnp.concatenate([res8, pltpu.roll(res8, 4, 0)], axis=1)
    rep = jnp.broadcast_to(res_rows.reshape(8, 1, 256), (8, 8, 256)).reshape(64, 256)
    diag = (i64 % 8) == (n64 % 8)
    mine = jnp.where(iota((8, 256), 1) // 8 == tp, 1.0, 0.0).astype(BF16)
    res_mine = dot(mine, jnp.where(diag, rep, 0.0).astype(BF16), NT)[0:1]
    fold = jnp.where(iota((32, 256), 1) // 8 == iota((32, 256), 0), 1.0, 0.0).astype(BF16)

    sent(5, buf6.at[pl.ds(0, NTP - 1)])
    arrived(6, buf7.at[pl.ds(0, NKV - 1)])
    gs = jnp.sum(buf7[...].astype(F32), axis=0)
    tail = gs[:, 256:]
    sq2 = jnp.sum(
        jnp.where((lane_t == FF_DEV) | (lane_t == FF_DEV + 1), tail, 0.0), axis=1, keepdims=True)
    rms2 = lax.rsqrt(sq2 * (1.0 / D) + EPS)
    gs = gs * jnp.concatenate([rms2[0:4], rms2[0:4]], axis=0)
    up = pltpu.roll(gs, 4, 0)
    hid = gs / (1.0 + jnp.exp(-gs)) * up
    hid = jnp.where((iota((8, FF_PAD), 1) < FF_DEV) & (iota((8, FF_PAD), 0) < 3), hid, 0.0)
    hid = jnp.broadcast_to(hid.reshape(8, 1, FF_PAD), (8, 8, FF_PAD)).reshape(64, FF_PAD)
    down = dot(hid.astype(BF16), wd[...], NN)
    down = jnp.where(diag, down, 0.0)
    d_hi = down.astype(BF16)
    d_lo = (down - d_hi.astype(F32)).astype(BF16)
    parts = dot(fold, d_hi, NT) + dot(fold, d_lo, NT)
    parts = jnp.concatenate([parts, jnp.zeros((32, 64), F32)], axis=1)
    stage8[...] = parts
    send(7, "tp", (), lambda p: stage8.at[pl.ds(p, 1)], buf8.at[pl.ds(tp, 1)])
    buf8[pl.ds(tp, 1)] = stage8[pl.ds(tp, 1)]
    sent(6, buf7.at[pl.ds(0, NKV - 1)])
    arrived(7, buf8.at[pl.ds(0, NTP - 1)])
    share = jnp.sum(buf8[...], axis=0, keepdims=True)[:, :64] + res_mine
    out[...] = jnp.concatenate([share[:, 0:8], share[:, 8:16], share[:, 16:24]], axis=0).astype(BF16)
    sent(7, buf8.at[pl.ds(0, NTP - 1)])


def body(
    tokens, lengths, attn_gain, w_query, w_key, w_value, w_forget, forget_bias,
    cache_keys, cache_values, cache_decay, out_gain, w_out, mlp_gain, w_gate, w_up, w_down,
):
    hbm = pl.BlockSpec(memory_space=pl.ANY)
    v = pltpu.VMEM
    return pl.pallas_call(
        kernel,
        out_shape=pltpu.VMEM((3, 8), BF16),
        in_specs=[hbm] * 17,
        out_specs=pl.BlockSpec(memory_space=pltpu.VMEM),
        scratch_shapes=[
            pltpu.SMEM((3,), jnp.int32), v((3, 8), BF16), v((1, 8), F32), v((1, 8), F32), v((1, 32), F32), v((16, 128), F32),
            v((128, 256), BF16), v((256, 128), BF16), v((256, 128), BF16), v((256, 128), BF16),
            v((3, 128, SPAN), BF16), v((3, 128, SPAN), BF16), v((3, 32, SPAN), F32),
            v((128, 256), BF16),
            v((FF_PAD, 256), BF16), v((FF_PAD, 256), BF16), v((FF_PAD, 256), BF16),
            v((NTP, 1, 128), F32), v((NKV, 8, 128), F32), v((3, NTP, 128), F32),
            v((3, NTP, 128), F32), v((3, NTP, 128), F32), v((3, NKV, 128), F32),
            v((NTP, 8, 128), BF16), v((NKV, 8, FF_PAD), BF16),
            v((NTP, 128), F32), v((NTP, 128), F32),
            pltpu.SemaphoreType.DMA((17,)),
            pltpu.SemaphoreType.DMA((8,)),
            pltpu.SemaphoreType.DMA((8,)),
            pltpu.SemaphoreType.REGULAR,
        ],
        compiler_params=pltpu.CompilerParams(
            collective_id=0, has_side_effects=True, vmem_limit_bytes=60 * 1024 * 1024),
    )(
        lengths, tokens, attn_gain.reshape(1, 8), mlp_gain.reshape(1, 8),
        forget_bias.reshape(1, 32), out_gain.reshape(16, 128),
        w_query.T, w_key, w_value, w_forget.T, cache_keys, cache_values, cache_decay, w_out,
        w_gate.T, w_up.T, w_down,
    )


def solution(mesh):
    kvtp = ("kv", "tp")
    placed = (
        P(None, kvtp), P(), P(kvtp), P("kv", "tp"), P("kv", None), P("kv", None), P(), P(),
        P(None, None, kvtp), P(None, None, kvtp), P(None, None, kvtp), P(), P("tp", "kv"),
        P(kvtp), P("kv", "tp"), P("kv", "tp"), P("tp", "kv"),
    )
    return jax.shard_map(
        body, mesh=mesh, in_specs=placed, out_specs=P(None, kvtp), check_vma=False)
```
